512 devices in a mesh: ep: 32 (over z, core), tp: 16 (over y, x).
Axes of the slice: x: 4, y: 4, z: 16, core: 2. Of those that a mesh axis runs over, the one named last changes fastest.
Arguments:
- query_input: bfloat16 [16384, 2048], P('ep', 'tp'), may hold values from -6 to 6
- key_input: bfloat16 [16384, 1024], P('ep', 'tp'), may hold values from -6 to 6
- value_input: bfloat16 [16384, 1024], P('ep', 'tp'), may hold values from -64 to 64
- query_gain: float32 [64], replicated, may hold values from 0.5 to 6
- key_gain: float32 [64], replicated, may hold values from 0.5 to 6
- mixer_out: bfloat16 [2048, 4096], P(None, 'tp'), may hold values from -0.125 to 0.125
- moe_input: bfloat16 [8192, 4096], P('ep'), may hold values from -6 to 6
- moe_gain: float32 [4096], replicated, may hold values from 0.1 to 1.9
- routes: int32 [8192, 2], P('ep'), may hold values from 0 to 31, all different within a row; in each aligned block of 256 rows (0 to 255, 256 to 511, ...) at most 24 rows name the same one
- route_weight: float32 [8192, 2], P('ep'), may hold values from 0.1 to 1
- expert_gate: bfloat16 [32, 4096, 1024], P('ep', None, 'tp'), may hold values from -0.09375 to 0.09375
- expert_up: bfloat16 [32, 4096, 1024], P('ep', None, 'tp'), may hold values from -0.09375 to 0.09375
- expert_down: bfloat16 [32, 1024, 4096], P('ep', None, 'tp'), may hold values from -0.1875 to 0.1875
Outputs:
- attn_mixed: bfloat16 [16384, 4096], P('ep', 'tp')
- moe_out: bfloat16 [8192, 4096], P('ep', 'tp')
The draws below stay inside these ranges and needn't reach their ends.
Inputs may be any that keep to these rules, and one draw needn't show every extreme that they name: `routes`: each row names 2 different experts. In the rows of one index of ep (aligned blocks of 256 rows) no expert is named by more than 24 rows, and in every draw some block has an expert named by exactly 24 rows.
All inputs are finite; a program needn't handle non-finite values.
Results may differ from the reference program's by a relative error of at most 0.0095.
The reference program's roundings to bfloat16 on the way count: a program that leaves them out, or rounds other values in their place, can miss the bound.
Values may be sent and summed in bfloat16 or wider, within the bound.
No kernel may reach another device: no remote copies, remote signals or barrier semaphores. Data moves between devices by JAX's collectives and lax.ppermute only.
A program may use at most 64 MiB of HBM per device.

```python
import math
import jax
import jax.numpy as jnp
import numpy as np
from jax import lax

D = 4096
HEADS = 32
KV_HEADS = 16
HEAD_DIM = 64
FF = 1024
GRID_W = 64
TOP_K = 2
MOE_TOK = 256
SEQ_LEN = 16384
MOE_TOKENS = 8192
EXPERTS = 32
CAP = 24
N_EP = 32


def draw_query_input(key, part):
    column_count = HEADS * HEAD_DIM
    samples = jnp.clip(jax.random.normal(jax.random.fold_in(key, 101), (SEQ_LEN, column_count), jnp.float32), -6.0, 6.0)
    return samples.astype(jnp.bfloat16)


def draw_key_input(key, part):
    column_count = KV_HEADS * HEAD_DIM
    samples = jnp.clip(jax.random.normal(jax.random.fold_in(key, 202), (SEQ_LEN, column_count), jnp.float32), -6.0, 6.0)
    return samples.astype(jnp.bfloat16)


def draw_query_gain(key, part):
    spread = jax.random.uniform(jax.random.fold_in(key, 303), (HEAD_DIM,), jnp.float32, jnp.log(0.5), jnp.log(2.0))
    gains = jnp.exp(spread)
    return gains.astype(jnp.float32)


def draw_key_gain(key, part):
    spread = jax.random.uniform(jax.random.fold_in(key, 404), (HEAD_DIM,), jnp.float32, jnp.log(0.5), jnp.log(2.0))
    gains = jnp.exp(spread)
    return gains.astype(jnp.float32)


def block_levels(key, shape, pieces, least, high):
    def one(axis_at, blocks):
        heights = jax.random.uniform(jax.random.fold_in(jax.random.fold_in(key, 6), axis_at), (blocks,), jnp.float32, least / len(pieces), high / len(pieces))
        return jnp.repeat(jnp.exp(heights), shape[axis_at] // blocks).reshape((-1,) + (1,) * (len(shape) - axis_at - 1))

    factor_of = one(*pieces[0])
    for cut in pieces[1:]:
        factor_of = factor_of * one(*cut)
    return factor_of


def routed_block(stream_key, own, number, rows, amount, top, bound, skew):
    order = jax.random.permutation(stream_key, amount)
    packed, common = portions_of(amount, rows * top, bound, skew, True), portions_of(amount, rows * top, bound, skew, False)
    places = jnp.arange(amount)

    def named(tallies, rotation):
        used = int((tallies > 0).sum())
        fixed = max(1, used // 4)
        moved = fixed + (places - fixed + rotation * (used - fixed)) % max(1, amount - fixed)
        return jnp.zeros((amount,), jnp.int32).at[order[jnp.where(places < fixed, places, moved)]].set(jnp.asarray(tallies, jnp.int32))

    tallies = jnp.where(number % 4 == 0, named(packed, number // 4), named(common, number - number // 4 - 1))
    mixed = jax.random.permutation(jax.random.fold_in(own, 3), amount)
    source_of, sink = mixed[0:amount // 2 * 2:2], mixed[1:amount // 2 * 2:2]
    slack = jnp.minimum(tallies[source_of] - 1, bound - tallies[sink]) // 2
    slack = jnp.where((source_of == order[0]) | (sink == order[0]) | (tallies[sink] == 0), 0, jnp.maximum(slack, 0))
    moved = jax.random.randint(jax.random.fold_in(own, 4), (amount // 2,), 0, 1 << 20) % (slack + 1)
    tallies = tallies.at[source_of].add(-moved).at[sink].add(moved)
    labels = jnp.searchsorted(jnp.cumsum(tallies), jnp.arange(rows * top), side="right").astype(jnp.int32)
    listing = labels.reshape(top, rows).T
    listing = listing[jax.random.permutation(jax.random.fold_in(own, 1), rows)]
    rotation = jax.random.randint(jax.random.fold_in(own, 2), (rows, 1), 0, top)
    return jnp.take_along_axis(listing, (jnp.arange(top)[None, :] + rotation) % top, axis=1)


def portions_of(amount, total, reach, skew, full):
    weights = [(1 << 20) // math.isqrt(rank ** skew) + 1 for rank in range(1, amount + 1)]
    largest = reach if full else min(reach, max(-(-total // amount), total * weights[0] // sum(weights)))
    least = 1 if total - largest >= amount - 1 else 0
    counts, rest = [largest] + [least] * (amount - 1), total - largest - least * (amount - 1)
    while rest > 0:
        movable = [i for i in range(1, amount) if counts[i] < largest] or [i for i in range(1, amount) if counts[i] < reach]
        pool, left = sum([weights[i] for i in movable]), rest
        for i in movable:
            addition = min(reach - counts[i], max(1, left * weights[i] // pool), rest)
            counts[i] = counts[i] + addition
            rest = rest - addition
    return np.array(counts)


def scatter_about(stream_key, dims, scale, bound, cuts=(), held_as=jnp.bfloat16):
    result = jax.random.normal(stream_key, dims, jnp.float32) * scale
    if len(cuts) > 0:
        result = block_levels(stream_key, dims, cuts, -0.22, 0.18) * result
    return jnp.clip(result, min=-bound, max=bound).astype(held_as)


def setup_inputs(seed: int = 0) -> dict:
    streams_of = jax.random.split(jax.random.key(seed), 14)
    query_input = draw_query_input(jax.random.fold_in(streams_of[13], 71), 0)
    key_input = draw_key_input(jax.random.fold_in(streams_of[13], 71), 0)
    value_input = jnp.clip(jax.random.uniform(streams_of[2], (SEQ_LEN, KV_HEADS * HEAD_DIM), jnp.float32, -64.0, 64.0) * block_levels(streams_of[2], (SEQ_LEN, KV_HEADS * HEAD_DIM), ((0, 32), (1, 16)), -0.4, 0.0), -64.0, 64.0).astype(jnp.bfloat16)
    query_gain = draw_query_gain(jax.random.fold_in(streams_of[13], 71), 0)
    key_gain = draw_key_gain(jax.random.fold_in(streams_of[13], 71), 0)
    mixer_out = scatter_about(streams_of[5], (HEADS * HEAD_DIM, D), (HEADS * HEAD_DIM) ** -0.5, 0.125, ((1, 16),))
    moe_input = scatter_about(streams_of[6], (MOE_TOKENS, D), 1.0, 6.0, ((0, 32),))
    moe_gain = jnp.clip(1.0 + 0.18 * jax.random.normal(streams_of[7], (D,), jnp.float32), 0.1, 1.9)
    routes_keys = jax.random.split(jax.random.fold_in(streams_of[8], 1), MOE_TOKENS // MOE_TOK)
    routes_turns = jax.random.permutation(jax.random.fold_in(streams_of[8], 3), MOE_TOKENS // MOE_TOK)
    routes = jax.vmap(lambda own, number: routed_block(jax.random.fold_in(streams_of[8], 2), own, number, MOE_TOK, EXPERTS, TOP_K, CAP, 1))(routes_keys, routes_turns).reshape((MOE_TOKENS, TOP_K))
    route_weight = jnp.clip(jnp.exp(math.log(1.0) - 2.3025851 * jax.random.uniform(streams_of[9], (MOE_TOKENS, TOP_K), jnp.float32) ** block_levels(streams_of[9], (MOE_TOKENS, TOP_K), ((0, 32),), -0.2, 0.2)), 0.1, 1.0)
    expert_gate = scatter_about(streams_of[10], (EXPERTS, D, FF), D ** -0.5, 0.09375, ((0, 32), (2, 16)))
    expert_up = scatter_about(streams_of[11], (EXPERTS, D, FF), D ** -0.5, 0.09375, ((0, 32), (2, 16)))
    expert_down = scatter_about(streams_of[12], (EXPERTS, FF, D), FF ** -0.5, 0.1875, ((0, 32), (2, 16)))
    return {"query_input": query_input, "key_input": key_input, "value_input": value_input, "query_gain": query_gain, "key_gain": key_gain, "mixer_out": mixer_out, "moe_input": moe_input, "moe_gain": moe_gain, "routes": routes, "route_weight": route_weight, "expert_gate": expert_gate, "expert_up": expert_up, "expert_down": expert_down}


epsilon = 1e-06
base_theta = 10000.0

def rope_tables(positions, head_width):
    quarter = head_width // 4
    inverse = base_theta ** (-jnp.arange(quarter, dtype=jnp.float32) / quarter)
    grid_row = (positions // GRID_W).astype(jnp.float32)
    grid_col = (positions % GRID_W).astype(jnp.float32)
    angles = jnp.concatenate([grid_row[:, None] * inverse[None, :], grid_col[:, None] * inverse[None, :]], axis=1)
    return (jnp.cos(angles), jnp.sin(angles))

def head_norm(heads_in, gain):
    return heads_in * lax.rsqrt(lax.optimization_barrier(jnp.mean(heads_in * heads_in, axis=-1, keepdims=True)) + epsilon) * gain

def rotate(heads_in, cosine, sine_table):
    half_width = heads_in.shape[-1] // 2
    first_half = heads_in[..., :half_width]
    second_half = heads_in[..., half_width:]
    cos_rows = cosine[:, None, :]
    sin_rows = sine_table[:, None, :]
    return jnp.concatenate([first_half * cos_rows - second_half * sin_rows, first_half * sin_rows + second_half * cos_rows], axis=-1)

def slot_places(route_block, expert_count, capacity):
    flat_routes = route_block.reshape(-1)
    one_hot = (flat_routes[:, None] == jnp.arange(expert_count, dtype=jnp.int32)[None, :]).astype(jnp.int32)
    earlier = jnp.cumsum(one_hot, axis=0) - one_hot
    return (flat_routes * capacity + lax.optimization_barrier(jnp.sum(earlier * one_hot, axis=1))).astype(jnp.int32)

def fill_sources(places, token_count, top_count, slot_total):
    source_rows = jnp.full((slot_total,), token_count, jnp.int32)
    pair_rows = (jnp.arange(token_count * top_count, dtype=jnp.int32) // top_count).astype(jnp.int32)
    return source_rows.at[places].set(pair_rows)

def attend(query_rot, key_rot, value_input):
    seq_len = query_rot.shape[0]
    group_size = HEADS // KV_HEADS
    block_len = math.gcd(seq_len, 128)
    key_all = key_rot.astype(jnp.float32)
    value_all = value_input.astype(jnp.float32).reshape(seq_len, KV_HEADS, HEAD_DIM)
    blocks = query_rot.astype(jnp.float32).reshape(seq_len // block_len, block_len, KV_HEADS, group_size, HEAD_DIM)
    score_scale = HEAD_DIM ** (-0.5)

    def one_block(query_block):
        scores = jnp.einsum('qkgd,skd->kgqs', query_block, key_all) * score_scale
        largest = lax.optimization_barrier(jnp.max(scores, axis=-1, keepdims=True))
        weights = jnp.exp(scores - largest)
        denominator = lax.optimization_barrier(jnp.sum(weights, axis=-1))
        rounded = lax.optimization_barrier(weights.astype(jnp.bfloat16)).astype(jnp.float32)
        numerator = jnp.einsum('kgqs,skd->qkgd', rounded, value_all)
        return numerator / jnp.transpose(denominator, (2, 0, 1))[..., None]
    attended = lax.map(one_block, blocks)
    return attended.reshape(seq_len, HEADS * HEAD_DIM).astype(jnp.bfloat16)

def experts_layer(moe_input, moe_gain, routes, route_weight, expert_gate, expert_up, expert_down):
    features = moe_input.astype(jnp.float32)
    normed = (features * lax.rsqrt(lax.optimization_barrier(jnp.mean(features * features, axis=-1, keepdims=True)) + epsilon) * moe_gain).astype(jnp.bfloat16)
    blocks = normed.reshape(N_EP, MOE_TOK, D)
    places = jax.vmap(lambda route_block: slot_places(route_block, EXPERTS, CAP))(routes.reshape(N_EP, MOE_TOK, TOP_K))
    sources = jax.vmap(lambda place_row: fill_sources(place_row, MOE_TOK, TOP_K, EXPERTS * CAP))(places)
    padded = jnp.concatenate([blocks, jnp.zeros((N_EP, 1, D), jnp.bfloat16)], axis=1)
    gathered = jax.vmap(lambda padded_block, source_row: padded_block[source_row])(padded, sources)
    per_expert = gathered.reshape(N_EP, EXPERTS, CAP, D).transpose(1, 0, 2, 3).reshape(EXPERTS, N_EP * CAP, D)

    def one_expert(operands):
        expert_rows, gate_matrix, up_matrix, down_matrix = operands
        gate_hidden = jnp.dot(expert_rows, gate_matrix, preferred_element_type=jnp.float32)
        up_hidden = jnp.dot(expert_rows, up_matrix, preferred_element_type=jnp.float32)
        hidden = (jax.nn.silu(gate_hidden) * up_hidden).astype(jnp.bfloat16)
        return jnp.dot(hidden, down_matrix, preferred_element_type=jnp.float32).astype(jnp.bfloat16)
    outputs = lax.map(one_expert, (per_expert, expert_gate, expert_up, expert_down))
    returned = outputs.reshape(EXPERTS, N_EP, CAP, D).transpose(1, 0, 2, 3).reshape(N_EP, EXPERTS * CAP, D)
    picked = jax.vmap(lambda returned_block, place_row: returned_block[place_row])(returned, places)
    picked = picked.reshape(N_EP * MOE_TOK, TOP_K, D).astype(jnp.float32)
    shares = route_weight / lax.optimization_barrier(jnp.sum(route_weight, axis=-1, keepdims=True))
    return lax.optimization_barrier(jnp.sum(picked * shares[:, :, None], axis=1)).astype(jnp.bfloat16)

def reference(query_input, key_input, value_input, query_gain, key_gain, mixer_out, moe_input, moe_gain, routes, route_weight, expert_gate, expert_up, expert_down):
    seq_len = query_input.shape[0]
    positions = jnp.arange(seq_len, dtype=jnp.int32)
    cosine, sine_table = rope_tables(positions, HEAD_DIM)
    query_heads = query_input.astype(jnp.float32).reshape(seq_len, HEADS, HEAD_DIM)
    key_heads = key_input.astype(jnp.float32).reshape(seq_len, KV_HEADS, HEAD_DIM)
    query_rot = rotate(head_norm(query_heads, query_gain), cosine, sine_table).astype(jnp.bfloat16)
    key_rot = rotate(head_norm(key_heads, key_gain), cosine, sine_table).astype(jnp.bfloat16)
    attended = attend(query_rot, key_rot, value_input)
    attn_mixed = jnp.dot(attended, mixer_out, preferred_element_type=jnp.float32).astype(jnp.bfloat16)
    moe_out = experts_layer(moe_input, moe_gain, routes, route_weight, expert_gate, expert_up, expert_down)
    return (attn_mixed, moe_out)
```

```python
import jax
import jax.numpy as jnp
from jax import lax
from jax.experimental import pallas as pl
from jax.experimental.pallas import tpu as pltpu
from jax.sharding import Mesh
from jax.sharding import PartitionSpec as P

GRID_W = 64
EP = ("z", "core")
TP = ("y", "x")
EPS = 1e-06
BASE = 10000.0
LOG2E = 1.4426950408889634

bf16 = jnp.bfloat16
f32 = jnp.float32


def dot(a, b):
    return jnp.dot(a, b, preferred_element_type=f32)


def params(mib=16):
    return pltpu.CompilerParams(vmem_limit_bytes=mib << 20)


def start_copies(pairs, sems):
    copies = [pltpu.make_async_copy(a, b, sems.at[i]) for i, (a, b) in enumerate(pairs)]
    for copy in copies:
        copy.start()
    return copies


def norm_turn(x, gain, cos, sin):
    half = x.shape[0] // 2
    x = x * lax.rsqrt(jnp.mean(x * x, axis=0, keepdims=True) + EPS) * gain
    a, b = x[:half], x[half:]
    return jnp.concatenate([a * cos - b * sin, a * sin + b * cos], axis=0)


def column(row):
    n = row.shape[1]
    same = lax.broadcasted_iota(jnp.int32, (n, n), 0) == lax.broadcasted_iota(
        jnp.int32, (n, n), 1
    )
    return jnp.sum(jnp.where(same, row, 0.0), axis=1, keepdims=True)


def key_body(
    k_hbm, v_hbm, gain_hbm, cos_ref, sin_ref, chunk_ref, k_ref, v_ref, gain_ref, sems
):
    for copy in start_copies(((k_hbm, k_ref), (v_hbm, v_ref), (gain_hbm, gain_ref)), sems):
        copy.wait()
    hw, n = k_ref.shape
    k_t = norm_turn(k_ref[...].astype(f32), column(gain_ref[...]), cos_ref[...], sin_ref[...])
    k_t = k_t.astype(bf16).astype(f32)
    packed = jnp.concatenate([k_t[:, : n // 2], k_t[:, n // 2 :]], axis=0)
    chunk_ref[: n // 2, :] = packed.T.astype(bf16)
    for j in range(n // 128):
        chunk_ref[n // 2 + hw * j : n // 2 + hw * (j + 1), :] = v_ref[:, 128 * j : 128 * (j + 1)]


def query_body(q_ref, gain_ref, cos_ref, sin_ref, qt_ref):
    n = q_ref.shape[0]
    hw = gain_ref.shape[1]
    q_t = q_ref[...].astype(f32).T
    gain = column(gain_ref[...])
    for h in range(q_t.shape[0] // hw):
        turned = norm_turn(q_t[hw * h : hw * (h + 1)], gain, cos_ref[...], sin_ref[...])
        scaled = turned.astype(bf16).astype(f32) * (hw**-0.5)
        qt_ref[:, n * h : n * (h + 1)] = scaled.astype(bf16)


def attend_body(
    qt_ref, kv_ref, out_ref, qlo_ref, qhi_ref, m_ref, acc_ref, s_ref, p_ref, *, n, hw, tile
):
    step = pl.program_id(0)
    cols = qt_ref.shape[1]
    half = n // 2

    @pl.when(step == 0)
    def _():
        zero = jnp.zeros((hw, cols), bf16)
        qlo_ref[:hw, :] = qt_ref[...]
        qlo_ref[hw:, :] = zero
        qhi_ref[:hw, :] = zero
        qhi_ref[hw:, :] = qt_ref[...]
        m_ref[...] = jnp.full(m_ref.shape, -1e30, f32)
        acc_ref[...] = jnp.zeros(acc_ref.shape, f32)

    ones = jnp.ones((16, half), bf16)
    units = [(c, t) for c in range(kv_ref.shape[0] // n) for t in range(cols // tile)]
    shrink = {}

    def scores(u):
        c, t = units[u]
        at = pl.ds(tile * t, tile)
        k_pack = kv_ref[n * c : n * c + half, :]
        s_ref[u % 2, :half, :] = dot(k_pack, qlo_ref[:, at])
        s_ref[u % 2, half:, :] = dot(k_pack, qhi_ref[:, at])

    def weights(u):
        at = pl.ds(tile * units[u][1], tile)
        s = s_ref[u % 2]
        old = m_ref[:, at]
        new = jnp.maximum(old, jnp.max(s, axis=0, keepdims=True) * LOG2E)
        m_ref[:, at] = new
        shrink[u] = jnp.exp2(old - new)
        p_ref[u % 2] = jnp.exp2(s * LOG2E - new).astype(bf16)

    def values(u):
        c, t = units[u]
        at = pl.ds(tile * t, tile)
        base = n * c + half
        v = [kv_ref[base + hw * j : base + hw * (j + 1), :] for j in range(4)]
        v_a = jnp.concatenate([jnp.concatenate(v[:2], axis=1), ones], axis=0)
        v_b = jnp.concatenate([jnp.concatenate(v[2:], axis=1), ones], axis=0)
        term = dot(v_a, p_ref[u % 2, :half, :]) + dot(v_b, p_ref[u % 2, half:, :])
        acc_ref[:, at] = acc_ref[:, at] * shrink[u] + term

    for i in range(len(units) + 2):
        if i < len(units):
            scores(i)
        if i >= 2:
            values(i - 2)
        if 1 <= i <= len(units):
            weights(i - 1)

    @pl.when(step == pl.num_programs(0) - 1)
    def _():
        acc = acc_ref[...]
        out = acc[:hw] / acc[hw : hw + 1]
        heads = cols // n
        stacked = jnp.concatenate([out[:, n * h : n * (h + 1)] for h in range(heads)], axis=0)
        out_ref[...] = stacked.T.astype(bf16)


def weights_body(at_ref, w0, w1, w2, w3, after_ref, out_ref):
    del after_ref
    x = at_ref[1]
    count = out_ref.shape[0]
    width = out_ref.shape[1] // count
    for j, w_ref in enumerate((w0, w1, w2, w3)):
        for d in range(count):
            row = pl.multiple_of((x ^ d) * width, width)
            out_ref[j, width * d : width * (d + 1), :] = w_ref[pl.ds(row, width), :]


def mixer_body(a0, a1, a2, a3, w_ref, own_ref, p1_ref, p2_ref, p3_ref):
    near = jnp.concatenate([a0[...], a1[...]], axis=1)
    far = jnp.concatenate([a2[...], a3[...]], axis=1)
    half = near.shape[1]
    for j, out_ref in enumerate((own_ref, p1_ref, p2_ref, p3_ref)):
        acc = dot(near, w_ref[j, :half, :]) + dot(far, w_ref[j, half:, :])
        out_ref[...] = acc.astype(out_ref.dtype)


def mixed_body(own_ref, r1_ref, r2_ref, r3_ref, out_ref):
    total = own_ref[...]
    for ref in (r1_ref, r2_ref, r3_ref):
        total = total + ref[...].astype(f32)
    out_ref[...] = total.astype(bf16)


def dispatch_body(
    at_ref, x_hbm, gain_hbm, routes_hbm, out_ref, x_ref, gain_ref, routes_ref, sems, *, experts, cap
):
    pairs = ((routes_hbm, routes_ref), (x_hbm, x_ref), (gain_hbm, gain_ref))
    copies = start_copies(pairs, sems)
    rows = x_ref.shape[0]
    copies[0].wait()
    ids = lax.broadcasted_iota(jnp.int32, (experts, rows), 0)
    hits = jnp.zeros((experts, rows), f32)
    for k in range(routes_ref.shape[0]):
        hits = hits + (ids == routes_ref[k : k + 1, :]).astype(f32)
    before = lax.broadcasted_iota(jnp.int32, (rows, rows), 0) < lax.broadcasted_iota(
        jnp.int32, (rows, rows), 1
    )
    rank = dot(hits.astype(bf16), before.astype(f32).astype(bf16))
    marks = (hits * (rank + 1.0)).astype(bf16)
    slots = experts * cap
    slot_row = lax.broadcasted_iota(jnp.int32, (slots, experts), 0)
    slot_exp = lax.broadcasted_iota(jnp.int32, (slots, experts), 1)
    spread = ((slot_row >= slot_exp * cap) & (slot_row < (slot_exp + 1) * cap)).astype(f32)
    wide = dot(spread.astype(bf16), marks)
    place = lax.broadcasted_iota(jnp.int32, (slots, rows), 0)
    want = (lax.rem(place, jnp.full_like(place, cap)) + 1).astype(f32)
    pick = (wide == want).astype(f32).astype(bf16)
    copies[1].wait()
    copies[2].wait()
    x = x_ref[...].astype(f32)
    width = out_ref.shape[1]
    own = pl.ds(pl.multiple_of(at_ref[0] * width, width), width)
    scale = lax.rsqrt(jnp.mean(x * x, axis=-1, keepdims=True) + EPS)
    normed = (x_ref[:, own].astype(f32) * scale * gain_ref[:, own]).astype(bf16)
    out_ref[...] = dot(pick, normed).astype(bf16)


def spread_body(x_ref, *refs):
    out_ref = refs[-1]
    cores, copies = 2, out_ref.shape[0] // 2
    count, rows, width = x_ref.shape
    cap = rows // cores
    x = x_ref[...].astype(f32)
    for c in range(cores):
        part = x[:, cap * c : cap * (c + 1), :].reshape(count * cap, width).astype(bf16)
        for i in range(copies):
            out_ref[copies * c + i] = part


def gate_up_body(at_ref, x_ref, w0_ref, w1_ref, w2_ref, w3_ref, *refs):
    out_ref = refs[-1]
    _, rows, width = x_ref.shape
    y = at_ref[0]
    ws = (w0_ref, w1_ref, w2_ref, w3_ref)
    blocks = w0_ref.shape[1] // width
    for j in range(0, len(ws), 2):
        for c in range(x_ref.shape[0] // blocks):
            acc = None
            for b in range(blocks):
                cols = slice(width * b, width * (b + 1))
                w = jnp.concatenate([ws[j][:, cols], ws[j + 1][:, cols]], axis=0)
                term = lax.dot_general(
                    x_ref[blocks * c + b], w, (((1,), (1,)), ((), ())), preferred_element_type=f32
                )
                acc = term if acc is None else acc + term
            half = acc.shape[1] // 2
            at = slice(rows * c, rows * (c + 1))
            out_ref[y ^ j, at, :] = acc[:, :half].astype(bf16)
            out_ref[y ^ (j + 1), at, :] = acc[:, half:].astype(bf16)


def hidden_body(parts_ref, out_ref):
    total = parts_ref[0].astype(f32)
    for j in range(1, parts_ref.shape[0]):
        total = total + parts_ref[j].astype(f32)
    hid = total.shape[1] // 2
    gate = total
    up = pltpu.roll(total, hid, 1)
    value = gate / (1.0 + jnp.exp(-gate)) * up
    rows = total.shape[0] // 2
    low = lax.broadcasted_iota(jnp.int32, (rows, 2 * hid), 1) < hid
    packed = jnp.where(low, value[:rows], pltpu.roll(value[rows:], hid, 1)).astype(bf16)
    for i in range(out_ref.shape[0]):
        out_ref[i] = packed


def down_body(h_ref, w_ref, after_ref, out_ref, wlo_ref, whi_ref):
    del after_ref
    count, rows, width = h_ref.shape
    hid = width // 2
    zero = jnp.zeros((hid, w_ref.shape[1]), bf16)
    for j in range(count):
        part = w_ref[hid * j : hid * (j + 1), :]
        wlo_ref[width * j : width * j + hid, :] = part
        wlo_ref[width * j + hid : width * (j + 1), :] = zero
        whi_ref[width * j : width * j + hid, :] = zero
        whi_ref[width * j + hid : width * (j + 1), :] = part
    top = bottom = None
    for j in range(0, count, 2):
        pair = jnp.concatenate([h_ref[j], h_ref[j + 1]], axis=1)
        a = dot(pair, wlo_ref[width * j : width * (j + 2), :])
        b = dot(pair, whi_ref[width * j : width * (j + 2), :])
        top = a if top is None else top + a
        bottom = b if bottom is None else bottom + b
    groups, both, width = out_ref.shape
    cap = both // 2
    out_ref[:, :cap, :] = top.reshape(groups, cap, width).astype(bf16)
    out_ref[:, cap:, :] = bottom.reshape(groups, cap, width).astype(bf16)


def routing_body(routes_ref, weight_ref, pick_ref, share_ref, *, experts, cap):
    top_k, rows = routes_ref.shape
    both = jnp.concatenate(
        [routes_ref[...].astype(f32), weight_ref[...], jnp.zeros((128 - 2 * top_k, rows), f32)],
        axis=0,
    ).T
    named = [both[:, k : k + 1].astype(jnp.int32) for k in range(top_k)]
    ids = lax.broadcasted_iota(jnp.int32, (rows, experts), 1)
    each = [(ids == name).astype(f32) for name in named]
    hits = each[0]
    total = both[:, top_k : top_k + 1]
    for k in range(1, top_k):
        hits = hits + each[k]
        total = total + both[:, top_k + k : top_k + k + 1]
    before = lax.broadcasted_iota(jnp.int32, (rows, rows), 1) < lax.broadcasted_iota(
        jnp.int32, (rows, rows), 0
    )
    rank = dot(before.astype(f32).astype(bf16), hits.astype(bf16))
    lane = lax.broadcasted_iota(jnp.int32, (rows, experts * cap), 1)
    for k in range(top_k):
        own_rank = jnp.sum(rank * each[k], axis=-1, keepdims=True).astype(jnp.int32)
        place = named[k] * cap + own_rank
        pick_ref[k] = (lane == place).astype(f32).astype(bf16)
        share = both[:, top_k + k : top_k + k + 1] / total
        share_ref[k] = jnp.broadcast_to(share, share_ref.shape[1:])


def combine_body(back_ref, pick_ref, share_ref, out_ref):
    back = back_ref[...]
    out = None
    for k in range(pick_ref.shape[0]):
        share = share_ref[k]
        share = jnp.concatenate([share] * (back.shape[1] // share.shape[1]), axis=1)
        term = dot(pick_ref[k], back) * share
        out = term if out is None else out + term
    out_ref[...] = out.astype(bf16)


def on_device(
    query_input,
    key_input,
    value_input,
    query_gain,
    key_gain,
    mixer_out,
    moe_input,
    moe_gain,
    routes,
    route_weight,
    expert_gate,
    expert_up,
    expert_down,
):
    seq, q_cols = query_input.shape
    hw = query_gain.shape[0]
    tokens, model = moe_input.shape
    tp = lax.axis_size(TP)
    ep = lax.axis_size(EP)
    ny = lax.axis_size("y")
    nx = lax.axis_size("x")
    width = model // tp
    experts = ep
    cap = 3 * tokens * routes.shape[1] // (2 * experts)
    slots = experts * cap
    hid = expert_gate.shape[2]

    at_y, at_x = lax.axis_index("y"), lax.axis_index("x")
    at_yx = jnp.stack([at_y, at_x]).astype(jnp.int32)
    smem = pl.BlockSpec(memory_space=pltpu.SMEM)
    vmem = pl.BlockSpec(memory_space=pltpu.VMEM)
    hbm = pl.BlockSpec(memory_space=pltpu.HBM)
    anywhere = pl.BlockSpec(memory_space=pl.ANY)

    positions = lax.axis_index(EP) * seq + jnp.arange(seq, dtype=jnp.int32)
    quarter = hw // 4
    inverse = BASE ** (-jnp.arange(quarter, dtype=f32) / quarter)
    row = (positions // GRID_W).astype(f32)
    col = (positions % GRID_W).astype(f32)
    angles = jnp.concatenate(
        [inverse[:, None] * row[None, :], inverse[:, None] * col[None, :]], axis=0
    )
    cos, sin = jnp.cos(angles), jnp.sin(angles)
    chunk = pl.pallas_call(
        key_body,
        out_shape=jax.ShapeDtypeStruct((seq, 2 * hw), bf16),
        in_specs=[hbm, hbm, hbm, vmem, vmem],
        scratch_shapes=[
            pltpu.VMEM((hw, seq), bf16),
            pltpu.VMEM((hw, seq), bf16),
            pltpu.VMEM((1, hw), f32),
            pltpu.SemaphoreType.DMA((3,)),
        ],
        compiler_params=params(60),
        name="keys",
    )(key_input.T, value_input.T, key_gain[None, :], cos, sin)
    keys = lax.all_gather(chunk, EP, axis=0, tiled=True)

    own = pl.pallas_call(
        lambda *refs: dispatch_body(*refs, experts=experts, cap=cap),
        out_shape=jax.ShapeDtypeStruct((slots, width), bf16),
        in_specs=[smem, hbm, hbm, hbm],
        scratch_shapes=[
            pltpu.VMEM((tokens, model), bf16),
            pltpu.VMEM((1, model), f32),
            pltpu.VMEM((routes.shape[1], tokens), jnp.int32),
            pltpu.SemaphoreType.DMA((3,)),
        ],
        compiler_params=params(60),
        name="dispatch",
    )(lax.axis_index(TP)[None].astype(jnp.int32), moe_input, moe_gain[None, :], routes.T)
    nz = lax.axis_size("z")
    received = lax.all_to_all(
        own.reshape(nz, 2 * cap, width), "z", split_axis=0, concat_axis=0, tiled=True
    )

    q_t = pl.pallas_call(
        query_body,
        out_shape=jax.ShapeDtypeStruct((hw, seq * q_cols // hw), bf16),
        compiler_params=params(),
        name="queries",
    )(query_input, query_gain[None, :], cos, sin)
    both = jnp.concatenate([expert_gate[0].T, expert_up[0].T], axis=0)
    deep = model // ny
    gate_up = []
    for d in range(ny):
        part = lax.dynamic_slice_in_dim(both, (at_y ^ d) * deep, deep, 1)
        if d:
            part = lax.ppermute(part, "y", [(i, i ^ d) for i in range(ny)])
        gate_up.append(part)
    pick, share = pl.pallas_call(
        lambda *refs: routing_body(*refs, experts=experts, cap=cap),
        out_shape=(
            jax.ShapeDtypeStruct((routes.shape[1], tokens, slots), bf16),
            jax.ShapeDtypeStruct((routes.shape[1], tokens, 128), f32),
        ),
        compiler_params=params(),
        name="routing",
    )(routes.T, route_weight.T)

    block = pl.pallas_call(
        spread_body,
        out_shape=jax.ShapeDtypeStruct((2 * nx, slots // 2, width), bf16),
        in_specs=[vmem] + [anywhere] * 5,
        compiler_params=params(),
        name="spread",
    )(received, *gate_up[1:], q_t, pick)
    block = lax.all_to_all(block, ("core", "x"), split_axis=0, concat_axis=0, tiled=True)
    rows_y = mixer_out.shape[0] // ny
    mixer = []
    for d in range(ny):
        part = lax.dynamic_slice_in_dim(mixer_out, (at_y ^ d) * rows_y, rows_y, 0)
        if d:
            part = lax.ppermute(part, "y", [(i, i ^ d) for i in range(ny)])
        mixer.append(part)

    partial = pl.pallas_call(
        gate_up_body,
        out_shape=jax.ShapeDtypeStruct((ny, slots, 2 * hid), bf16),
        in_specs=[smem] + [vmem] * 5 + [anywhere],
        compiler_params=params(),
        name="gate_up",
    )(at_yx, block, *gate_up, sum(part[:8, :128] for part in mixer[1:]))
    partial = lax.all_to_all(partial, "y", split_axis=0, concat_axis=0, tiled=True)
    hidden = pl.pallas_call(
        hidden_body,
        out_shape=jax.ShapeDtypeStruct((tp, slots // 2, 2 * hid), bf16),
        compiler_params=params(),
        name="hidden",
    )(partial)
    all_hidden = lax.all_to_all(hidden, TP, split_axis=0, concat_axis=0, tiled=True)

    step_rows = 4 * seq
    attended = pl.pallas_call(
        lambda *refs: attend_body(*refs, n=seq, hw=hw, tile=256),
        out_shape=jax.ShapeDtypeStruct((seq, q_cols), bf16),
        grid=(ep * seq // step_rows,),
        in_specs=[
            pl.BlockSpec(q_t.shape, lambda i: (0, 0)),
            pl.BlockSpec((step_rows, 2 * hw), lambda i: (i, 0)),
        ],
        out_specs=pl.BlockSpec((seq, q_cols), lambda i: (0, 0)),
        scratch_shapes=[
            pltpu.VMEM((2 * hw, q_t.shape[1]), bf16),
            pltpu.VMEM((2 * hw, q_t.shape[1]), bf16),
            pltpu.VMEM((1, q_t.shape[1]), f32),
            pltpu.VMEM((hw + 16, q_t.shape[1]), f32),
            pltpu.VMEM((2, seq, 256), f32),
            pltpu.VMEM((2, seq, 256), bf16),
        ],
        compiler_params=params(32),
        cost_estimate=pl.CostEstimate(
            flops=4 * seq * seq * ep * q_cols, bytes_accessed=4 << 20, transcendentals=0
        ),
        name="attend",
    )(q_t, keys)
    parts = [attended]
    for d in range(1, nx):
        parts.append(lax.ppermute(attended, "x", [(i, i ^ d) for i in range(nx)]))

    expert_out = pl.pallas_call(
        down_body,
        out_shape=jax.ShapeDtypeStruct((nz, 2 * cap, width), bf16),
        in_specs=[vmem, vmem, anywhere],
        scratch_shapes=[
            pltpu.VMEM((2 * hid * tp, width), bf16),
            pltpu.VMEM((2 * hid * tp, width), bf16),
        ],
        compiler_params=params(),
        name="down",
    )(all_hidden, expert_down[0], attended)
    returned = lax.all_to_all(
        expert_out.reshape(ep, cap, width), EP, split_axis=0, concat_axis=0, tiled=True
    ).reshape(slots, width)

    features = mixer_out.shape[1]
    turned = pl.pallas_call(
        weights_body,
        out_shape=jax.ShapeDtypeStruct((ny, rows_y, features), bf16),
        in_specs=[smem] + [vmem] * 4 + [anywhere],
        compiler_params=params(),
        name="weights",
    )(at_yx, *mixer, attended[:8, :])
    mixed = pl.pallas_call(
        mixer_body,
        out_shape=[jax.ShapeDtypeStruct((seq, features), f32)]
        + [jax.ShapeDtypeStruct((seq, features), bf16)] * (ny - 1),
        compiler_params=params(),
        name="mixer",
    )(*parts, turned)
    sums = [mixed[0]]
    for d in range(1, ny):
        sums.append(lax.ppermute(mixed[d], "y", [(i, i ^ d) for i in range(ny)]))
    attn_mixed = pl.pallas_call(
        mixed_body,
        out_shape=jax.ShapeDtypeStruct((seq, features), bf16),
        compiler_params=params(),
        name="mixed",
    )(*sums)

    moe_out = pl.pallas_call(
        combine_body,
        out_shape=jax.ShapeDtypeStruct((tokens, width), bf16),
        compiler_params=params(),
        name="combine",
    )(returned, pick, share)
    return (attn_mixed, moe_out)


def solution(mesh):
    torus = Mesh(mesh.devices.reshape(mesh.shape["ep"] // 2, 2, 4, 4), (*EP, *TP))
    placed = (
        P(EP, TP),
        P(EP, TP),
        P(EP, TP),
        P(),
        P(),
        P(None, TP),
        P(EP, None),
        P(),
        P(EP, None),
        P(EP, None),
        P(EP, None, TP),
        P(EP, None, TP),
        P(EP, None, TP),
    )
    return jax.shard_map(
        on_device,
        mesh=torus,
        in_specs=placed,
        out_specs=(P(EP, TP), P(EP, TP)),
        check_vma=False,
    )
```

```python
import jax
import jax.numpy as jnp
from jax import lax
from jax.experimental import pallas as pl
from jax.experimental.pallas import tpu as pltpu
from jax.sharding import Mesh
from jax.sharding import PartitionSpec as P


GRID_W = 64
EP = ("z", "core")
TP = ("y", "x")
EPS = 1e-06
BASE = 10000.0
LOG2E = 1.4426950408889634

bf16 = jnp.bfloat16
f32 = jnp.float32


def dot(a, b):
    return jnp.dot(a, b, preferred_element_type=f32)


def params(mib=16):
    return pltpu.CompilerParams(vmem_limit_bytes=mib << 20)


def start_copies(pairs, sems):
    copies = [pltpu.make_async_copy(a, b, sems.at[i]) for i, (a, b) in enumerate(pairs)]
    for copy in copies:
        copy.start()
    return copies


def norm_turn(x, gain, cos, sin):
    half = x.shape[0] // 2
    x = x * lax.rsqrt(jnp.mean(x * x, axis=0, keepdims=True) + EPS) * gain
    a, b = x[:half], x[half:]
    return jnp.concatenate([a * cos - b * sin, a * sin + b * cos], axis=0)


def column(row):
    n = row.shape[1]
    same = lax.broadcasted_iota(jnp.int32, (n, n), 0) == lax.broadcasted_iota(
        jnp.int32, (n, n), 1
    )
    return jnp.sum(jnp.where(same, row, 0.0), axis=1, keepdims=True)


def key_body(
    k_hbm, v_hbm, gain_hbm, cos_ref, sin_ref, chunk_ref, k_ref, v_ref, gain_ref, sems
):
    for copy in start_copies(((k_hbm, k_ref), (v_hbm, v_ref), (gain_hbm, gain_ref)), sems):
        copy.wait()
    hw, n = k_ref.shape
    k_t = norm_turn(k_ref[...].astype(f32), column(gain_ref[...]), cos_ref[...], sin_ref[...])
    k_t = k_t.astype(bf16).astype(f32)
    packed = jnp.concatenate([k_t[:, : n // 2], k_t[:, n // 2 :]], axis=0)
    chunk_ref[: n // 2, :] = packed.T.astype(bf16)
    for j in range(n // 128):
        chunk_ref[n // 2 + hw * j : n // 2 + hw * (j + 1), :] = v_ref[:, 128 * j : 128 * (j + 1)]


def query_body(q_ref, gain_ref, cos_ref, sin_ref, qt_ref):
    n = q_ref.shape[0]
    hw = gain_ref.shape[1]
    q_t = q_ref[...].astype(f32).T
    gain = column(gain_ref[...])
    for h in range(q_t.shape[0] // hw):
        turned = norm_turn(q_t[hw * h : hw * (h + 1)], gain, cos_ref[...], sin_ref[...])
        scaled = turned.astype(bf16).astype(f32) * (hw**-0.5)
        qt_ref[:, n * h : n * (h + 1)] = scaled.astype(bf16)


def attend_body(
    qt_ref, kv_ref, out_ref, qlo_ref, qhi_ref, m_ref, acc_ref, s_ref, p_ref, *, n, hw, tile
):
    step = pl.program_id(0)
    cols = qt_ref.shape[1]
    half = n // 2

    @pl.when(step == 0)
    def _():
        zero = jnp.zeros((hw, cols), bf16)
        scaled = qt_ref[...].astype(f32) * LOG2E
        big = scaled.astype(bf16)
        small = (scaled - big.astype(f32)).astype(bf16)
        for place, part in enumerate((big, zero, small, zero)):
            qlo_ref[hw * place : hw * (place + 1), :] = part
        for place, part in enumerate((zero, big, zero, small)):
            qhi_ref[hw * place : hw * (place + 1), :] = part
        m_ref[...] = jnp.full(m_ref.shape, -1e30, f32)
        acc_ref[...] = jnp.zeros(acc_ref.shape, f32)

    ones = jnp.ones((16, half), bf16)
    units = [(c, t) for c in range(kv_ref.shape[0] // n) for t in range(cols // tile)]
    shrink = {}

    def scores(u):
        c, t = units[u]
        at = pl.ds(tile * t, tile)
        k_pack = kv_ref[n * c : n * c + half, :]
        k_pack = jnp.concatenate([k_pack, k_pack], axis=1)
        s_ref[u % 2, :half, :] = dot(k_pack, qlo_ref[:, at])
        s_ref[u % 2, half:, :] = dot(k_pack, qhi_ref[:, at])

    def weights(u):
        at = pl.ds(tile * units[u][1], tile)
        s = s_ref[u % 2]
        old = m_ref[:, at]
        new = jnp.maximum(old, jnp.max(s, axis=0, keepdims=True))
        m_ref[:, at] = new
        shrink[u] = jnp.exp2(old - new)
        p_ref[u % 2] = jnp.exp2(s - new).astype(bf16)

    def values(u):
        c, t = units[u]
        at = pl.ds(tile * t, tile)
        base = n * c + half
        v = [kv_ref[base + hw * j : base + hw * (j + 1), :] for j in range(4)]
        v_a = jnp.concatenate([jnp.concatenate(v[:2], axis=1), ones], axis=0)
        v_b = jnp.concatenate([jnp.concatenate(v[2:], axis=1), ones], axis=0)
        term = dot(v_a, p_ref[u % 2, :half, :]) + dot(v_b, p_ref[u % 2, half:, :])
        acc_ref[:, at] = acc_ref[:, at] * shrink[u] + term

    for i in range(len(units) + 2):
        if i < len(units):
            scores(i)
        if i >= 2:
            values(i - 2)
        if 1 <= i <= len(units):
            weights(i - 1)

    @pl.when(step == pl.num_programs(0) - 1)
    def _():
        acc = acc_ref[...]
        out = acc[:hw] / acc[hw : hw + 1]
        heads = cols // n
        stacked = jnp.concatenate([out[:, n * h : n * (h + 1)] for h in range(heads)], axis=0)
        out_ref[...] = stacked.T.astype(bf16)


def weights_body(at_ref, w0, w1, w2, w3, after_ref, out_ref):
    del after_ref
    x = at_ref[1]
    count = out_ref.shape[0]
    width = out_ref.shape[1] // count
    base = w0.shape[0] - out_ref.shape[1]
    for j, w_ref in enumerate((w0, w1, w2, w3)):
        for d in range(count):
            row = pl.multiple_of(base + (x ^ d) * width, width)
            out_ref[j, width * d : width * (d + 1), :] = w_ref[pl.ds(row, width), :]


def mixer_body(a0, a1, a2, a3, w_ref, own_ref, p1_ref, p2_ref, p3_ref):
    near = jnp.concatenate([a0[...], a1[...]], axis=1)
    far = jnp.concatenate([a2[...], a3[...]], axis=1)
    half = near.shape[1]
    for j, out_ref in enumerate((own_ref, p1_ref, p2_ref, p3_ref)):
        acc = dot(near, w_ref[j, :half, :]) + dot(far, w_ref[j, half:, :])
        out_ref[...] = acc.astype(out_ref.dtype)


def mixed_body(own_ref, r1_ref, r2_ref, r3_ref, out_ref):
    total = own_ref[...]
    for ref in (r1_ref, r2_ref, r3_ref):
        total = total + ref[...].astype(f32)
    out_ref[...] = total.astype(bf16)


def dispatch_body(
    at_ref, x_hbm, gain_hbm, routes_hbm, out_ref, x_ref, gain_ref, routes_ref, sems, *, experts, cap
):
    pairs = ((routes_hbm, routes_ref), (x_hbm, x_ref), (gain_hbm, gain_ref))
    copies = start_copies(pairs, sems)
    rows = x_ref.shape[0]
    copies[0].wait()
    ids = lax.broadcasted_iota(jnp.int32, (experts, rows), 0)
    hits = jnp.zeros((experts, rows), f32)
    for k in range(routes_ref.shape[0]):
        hits = hits + (ids == routes_ref[k : k + 1, :]).astype(f32)
    before = lax.broadcasted_iota(jnp.int32, (rows, rows), 0) < lax.broadcasted_iota(
        jnp.int32, (rows, rows), 1
    )
    rank = dot(hits.astype(bf16), before.astype(f32).astype(bf16))
    marks = (hits * (rank + 1.0)).astype(bf16)
    slots = experts * cap
    slot_row = lax.broadcasted_iota(jnp.int32, (slots, experts), 0)
    slot_exp = lax.broadcasted_iota(jnp.int32, (slots, experts), 1)
    spread = ((slot_row >= slot_exp * cap) & (slot_row < (slot_exp + 1) * cap)).astype(f32)
    wide = dot(spread.astype(bf16), marks)
    place = lax.broadcasted_iota(jnp.int32, (slots, rows), 0)
    want = (lax.rem(place, jnp.full_like(place, cap)) + 1).astype(f32)
    pick = (wide == want).astype(f32).astype(bf16)
    copies[1].wait()
    copies[2].wait()
    x = x_ref[...].astype(f32)
    width = out_ref.shape[1]
    own = pl.ds(pl.multiple_of(at_ref[0] * width, width), width)
    scale = lax.rsqrt(jnp.mean(x * x, axis=-1, keepdims=True) + EPS)
    normed = (x_ref[:, own].astype(f32) * scale * gain_ref[:, own]).astype(bf16)
    out_ref[...] = dot(pick, normed).astype(bf16)


def pack_body(at_ref, gate_ref, up_ref, mixer_ref, *out_refs):
    y = at_ref[0]
    count = len(out_refs)
    hid, width = gate_ref.shape[0], out_refs[0].shape[1]
    deep, rows = gate_ref.shape[1] // count, mixer_ref.shape[0] // count
    for d, out_ref in enumerate(out_refs):
        row = lax.rem(y + count - d, count)
        for b in range(deep // width):
            at = pl.ds(pl.multiple_of(row * deep + b * width, width), width)
            out_ref[2 * hid * b : 2 * hid * b + hid, :] = gate_ref[:, at]
            out_ref[2 * hid * b + hid : 2 * hid * (b + 1), :] = up_ref[:, at]
        out_ref[2 * hid * deep // width :, :] = mixer_ref[pl.ds(pl.multiple_of(row * rows, rows), rows), :]


def spread_body(x_ref, *refs):
    out_ref = refs[-1]
    cores, copies = 2, out_ref.shape[0] // 2
    count, rows, width = x_ref.shape
    cap = rows // cores
    x = x_ref[...].astype(f32)
    for c in range(cores):
        part = x[:, cap * c : cap * (c + 1), :].reshape(count * cap, width).astype(bf16)
        for i in range(copies):
            out_ref[copies * c + i] = part


def gate_up_body(at_ref, x_ref, w0_ref, w1_ref, w2_ref, w3_ref, out_ref):
    _, rows, _ = x_ref.shape
    y = at_ref[0]
    ws = (w0_ref, w1_ref, w2_ref, w3_ref)
    hid = out_ref.shape[2]
    blocks = x_ref.shape[0] // 2
    for j in range(0, len(ws), 2):
        for c in range(2):
            acc = None
            for b in range(blocks):
                at = slice(hid * b, hid * (b + 1))
                w = jnp.concatenate([ws[j][at, :], ws[j + 1][at, :]], axis=0)
                term = lax.dot_general(
                    x_ref[blocks * c + b], w, (((1,), (1,)), ((), ())), preferred_element_type=f32
                )
                acc = term if acc is None else acc + term
            at = slice(rows * c, rows * (c + 1))
            out_ref[lax.rem(y + j, len(ws)), at, :] = acc[:, :hid].astype(bf16)
            out_ref[lax.rem(y + j + 1, len(ws)), at, :] = acc[:, hid:].astype(bf16)


def hidden_body(parts_ref, out_ref):
    total = parts_ref[0].astype(f32)
    for j in range(1, parts_ref.shape[0]):
        total = total + parts_ref[j].astype(f32)
    hid = total.shape[1] // 2
    gate = total
    up = pltpu.roll(total, hid, 1)
    value = gate / (1.0 + jnp.exp(-gate)) * up
    rows = total.shape[0] // 2
    low = lax.broadcasted_iota(jnp.int32, (rows, 2 * hid), 1) < hid
    packed = jnp.where(low, value[:rows], pltpu.roll(value[rows:], hid, 1)).astype(bf16)
    for i in range(out_ref.shape[0]):
        out_ref[i] = packed


def down_body(h_ref, w_ref, after_ref, out_ref, wlo_ref, whi_ref):
    del after_ref
    count, _, width = h_ref.shape
    hid = width // 2
    zero = jnp.zeros((hid, w_ref.shape[1]), bf16)
    for j in range(count):
        part = w_ref[hid * j : hid * (j + 1), :]
        wlo_ref[width * j : width * j + hid, :] = part
        wlo_ref[width * j + hid : width * (j + 1), :] = zero
        whi_ref[width * j : width * j + hid, :] = zero
        whi_ref[width * j + hid : width * (j + 1), :] = part
    top = bottom = None
    for j in range(0, count, 2):
        pair = jnp.concatenate([h_ref[j], h_ref[j + 1]], axis=1)
        a = dot(pair, wlo_ref[width * j : width * (j + 2), :])
        b = dot(pair, whi_ref[width * j : width * (j + 2), :])
        top = a if top is None else top + a
        bottom = b if bottom is None else bottom + b
    groups, both, width = out_ref.shape
    cap = both // 2
    out_ref[:, :cap, :] = top.reshape(groups, cap, width).astype(bf16)
    out_ref[:, cap:, :] = bottom.reshape(groups, cap, width).astype(bf16)


def routing_body(routes_ref, weight_ref, pick_ref, share_ref, *, experts, cap):
    top_k, rows = routes_ref.shape
    both = jnp.concatenate(
        [routes_ref[...].astype(f32), weight_ref[...], jnp.zeros((128 - 2 * top_k, rows), f32)],
        axis=0,
    ).T
    named = [both[:, k : k + 1].astype(jnp.int32) for k in range(top_k)]
    ids = lax.broadcasted_iota(jnp.int32, (rows, experts), 1)
    each = [(ids == name).astype(f32) for name in named]
    hits = each[0]
    total = both[:, top_k : top_k + 1]
    for k in range(1, top_k):
        hits = hits + each[k]
        total = total + both[:, top_k + k : top_k + k + 1]
    before = lax.broadcasted_iota(jnp.int32, (rows, rows), 1) < lax.broadcasted_iota(
        jnp.int32, (rows, rows), 0
    )
    rank = dot(before.astype(f32).astype(bf16), hits.astype(bf16))
    lane = lax.broadcasted_iota(jnp.int32, (rows, experts * cap), 1)
    for k in range(top_k):
        own_rank = jnp.sum(rank * each[k], axis=-1, keepdims=True).astype(jnp.int32)
        place = named[k] * cap + own_rank
        pick_ref[k] = (lane == place).astype(f32).astype(bf16)
        share = both[:, top_k + k : top_k + k + 1] / total
        share_ref[k] = jnp.broadcast_to(share, share_ref.shape[1:])


def combine_body(back_ref, pick_ref, share_ref, out_ref):
    back = back_ref[...]
    out = None
    for k in range(pick_ref.shape[0]):
        share = share_ref[k]
        share = jnp.concatenate([share] * (back.shape[1] // share.shape[1]), axis=1)
        term = dot(pick_ref[k], back) * share
        out = term if out is None else out + term
    out_ref[...] = out.astype(bf16)


def on_device(
    query_input,
    key_input,
    value_input,
    query_gain,
    key_gain,
    mixer_out,
    moe_input,
    moe_gain,
    routes,
    route_weight,
    expert_gate,
    expert_up,
    expert_down,
):
    seq, q_cols = query_input.shape
    hw = query_gain.shape[0]
    tokens, model = moe_input.shape
    tp = lax.axis_size(TP)
    ep = lax.axis_size(EP)
    ny = lax.axis_size("y")
    nx = lax.axis_size("x")
    width = model // tp
    experts = ep
    cap = 3 * tokens * routes.shape[1] // (2 * experts)
    slots = experts * cap
    hid = expert_gate.shape[2]

    at_y, at_x = lax.axis_index("y"), lax.axis_index("x")
    at_yx = jnp.stack([at_y, at_x]).astype(jnp.int32)
    smem = pl.BlockSpec(memory_space=pltpu.SMEM)
    vmem = pl.BlockSpec(memory_space=pltpu.VMEM)
    hbm = pl.BlockSpec(memory_space=pltpu.HBM)
    anywhere = pl.BlockSpec(memory_space=pl.ANY)

    positions = lax.axis_index(EP) * seq + jnp.arange(seq, dtype=jnp.int32)
    quarter = hw // 4
    inverse = BASE ** (-jnp.arange(quarter, dtype=f32) / quarter)
    row = (positions // GRID_W).astype(f32)
    col = (positions % GRID_W).astype(f32)
    angles = jnp.concatenate(
        [inverse[:, None] * row[None, :], inverse[:, None] * col[None, :]], axis=0
    )
    cos, sin = jnp.cos(angles), jnp.sin(angles)
    chunk = pl.pallas_call(
        key_body,
        out_shape=jax.ShapeDtypeStruct((seq, 2 * hw), bf16),
        in_specs=[hbm, hbm, hbm, vmem, vmem],
        scratch_shapes=[
            pltpu.VMEM((hw, seq), bf16),
            pltpu.VMEM((hw, seq), bf16),
            pltpu.VMEM((1, hw), f32),
            pltpu.SemaphoreType.DMA((3,)),
        ],
        compiler_params=params(60),
        name="keys",
    )(key_input.T, value_input.T, key_gain[None, :], cos, sin)
    keys = lax.all_gather(chunk, EP, axis=0, tiled=True)

    own = pl.pallas_call(
        lambda *refs: dispatch_body(*refs, experts=experts, cap=cap),
        out_shape=jax.ShapeDtypeStruct((slots, width), bf16),
        in_specs=[smem, hbm, hbm, hbm],
        scratch_shapes=[
            pltpu.VMEM((tokens, model), bf16),
            pltpu.VMEM((1, model), f32),
            pltpu.VMEM((routes.shape[1], tokens), jnp.int32),
            pltpu.SemaphoreType.DMA((3,)),
        ],
        compiler_params=params(60),
        name="dispatch",
    )(lax.axis_index(TP)[None].astype(jnp.int32), moe_input, moe_gain[None, :], routes.T)
    nz = lax.axis_size("z")
    received = lax.all_to_all(
        own.reshape(nz, 2 * cap, width), "z", split_axis=0, concat_axis=0, tiled=True
    )

    q_t = pl.pallas_call(
        query_body,
        out_shape=jax.ShapeDtypeStruct((hw, seq * q_cols // hw), bf16),
        compiler_params=params(),
        name="queries",
    )(query_input, query_gain[None, :], cos, sin)
    rows_y = mixer_out.shape[0] // ny
    packs = pl.pallas_call(
        pack_body,
        out_shape=[jax.ShapeDtypeStruct((2 * hid * nx + rows_y, width), bf16)] * ny,
        in_specs=[smem] + [vmem] * 3,
        compiler_params=params(),
        name="pack",
    )(at_yx, expert_gate[0].T, expert_up[0].T, mixer_out)
    moved = [packs[0]]
    for d in range(1, ny):
        moved.append(lax.ppermute(packs[d], "y", [(i, (i - d) % ny) for i in range(ny)]))
    pick, share = pl.pallas_call(
        lambda *refs: routing_body(*refs, experts=experts, cap=cap),
        out_shape=(
            jax.ShapeDtypeStruct((routes.shape[1], tokens, slots), bf16),
            jax.ShapeDtypeStruct((routes.shape[1], tokens, 128), f32),
        ),
        compiler_params=params(),
        name="routing",
    )(routes.T, route_weight.T)

    block = pl.pallas_call(
        spread_body,
        out_shape=jax.ShapeDtypeStruct((2 * nx, slots // 2, width), bf16),
        in_specs=[vmem] + [anywhere] * 3,
        compiler_params=params(),
        name="spread",
    )(received, q_t, pick, packs[0][:8, :128])
    block = lax.all_to_all(block, ("core", "x"), split_axis=0, concat_axis=0, tiled=True)
    partial = pl.pallas_call(
        gate_up_body,
        out_shape=jax.ShapeDtypeStruct((ny, slots, 2 * hid), bf16),
        in_specs=[smem] + [vmem] * 5,
        compiler_params=params(),
        name="gate_up",
    )(at_yx, block, *moved)
    partial = lax.all_to_all(partial, "y", split_axis=0, concat_axis=0, tiled=True)
    hidden = pl.pallas_call(
        hidden_body,
        out_shape=jax.ShapeDtypeStruct((tp, slots // 2, 2 * hid), bf16),
        compiler_params=params(),
        name="hidden",
    )(partial)
    all_hidden = lax.all_to_all(hidden, TP, split_axis=0, concat_axis=0, tiled=True)

    step_rows = 8 * seq
    attended = pl.pallas_call(
        lambda *refs: attend_body(*refs, n=seq, hw=hw, tile=256),
        out_shape=jax.ShapeDtypeStruct((seq, q_cols), bf16),
        grid=(ep * seq // step_rows,),
        in_specs=[
            pl.BlockSpec(q_t.shape, lambda i: (0, 0)),
            pl.BlockSpec((step_rows, 2 * hw), lambda i: (i, 0)),
        ],
        out_specs=pl.BlockSpec((seq, q_cols), lambda i: (0, 0)),
        scratch_shapes=[
            pltpu.VMEM((4 * hw, q_t.shape[1]), bf16),
            pltpu.VMEM((4 * hw, q_t.shape[1]), bf16),
            pltpu.VMEM((1, q_t.shape[1]), f32),
            pltpu.VMEM((hw + 16, q_t.shape[1]), f32),
            pltpu.VMEM((2, seq, 256), f32),
            pltpu.VMEM((2, seq, 256), bf16),
        ],
        compiler_params=params(32),
        cost_estimate=pl.CostEstimate(
            flops=4 * seq * seq * ep * q_cols, bytes_accessed=4 << 20, transcendentals=0
        ),
        name="attend",
    )(q_t, keys)
    parts = [attended]
    for d in range(1, nx):
        parts.append(lax.ppermute(attended, "x", [(i, i ^ d) for i in range(nx)]))

    expert_out = pl.pallas_call(
        down_body,
        out_shape=jax.ShapeDtypeStruct((nz, 2 * cap, width), bf16),
        in_specs=[vmem, vmem, anywhere],
        scratch_shapes=[
            pltpu.VMEM((2 * hid * tp, width), bf16),
            pltpu.VMEM((2 * hid * tp, width), bf16),
        ],
        compiler_params=params(),
        name="down",
    )(all_hidden, expert_down[0], attended)
    returned = lax.all_to_all(
        expert_out.reshape(ep, cap, width), EP, split_axis=0, concat_axis=0, tiled=True
    ).reshape(slots, width)

    features = mixer_out.shape[1]
    turned = pl.pallas_call(
        weights_body,
        out_shape=jax.ShapeDtypeStruct((ny, rows_y, features), bf16),
        in_specs=[smem] + [vmem] * 4 + [anywhere],
        compiler_params=params(),
        name="weights",
    )(at_yx, *moved, attended[:8, :])
    mixed = pl.pallas_call(
        mixer_body,
        out_shape=[jax.ShapeDtypeStruct((seq, features), f32)]
        + [jax.ShapeDtypeStruct((seq, features), bf16)] * (ny - 1),
        compiler_params=params(),
        name="mixer",
    )(*parts, turned)
    sums = [mixed[0]]
    for d in range(1, ny):
        sums.append(lax.ppermute(mixed[d], "y", [(i, (i + d) % ny) for i in range(ny)]))
    attn_mixed = pl.pallas_call(
        mixed_body,
        out_shape=jax.ShapeDtypeStruct((seq, features), bf16),
        compiler_params=params(),
        name="mixed",
    )(*sums)

    moe_out = pl.pallas_call(
        combine_body,
        out_shape=jax.ShapeDtypeStruct((tokens, width), bf16),
        compiler_params=params(),
        name="combine",
    )(returned, pick, share)
    return (attn_mixed, moe_out)


def solution(mesh):
    torus = Mesh(mesh.devices.reshape(mesh.shape["ep"] // 2, 2, 4, 4), (*EP, *TP))
    placed = (
        P(EP, TP),
        P(EP, TP),
        P(EP, TP),
        P(),
        P(),
        P(None, TP),
        P(EP, None),
        P(),
        P(EP, None),
        P(EP, None),
        P(EP, None, TP),
        P(EP, None, TP),
        P(EP, None, TP),
    )

    return jax.shard_map(
        on_device,
        mesh=torus,
        in_specs=placed,
        out_specs=(P(EP, TP), P(EP, TP)),
        check_vma=False,
    )
```

```python
import jax
import jax.numpy as jnp
from jax import lax
from jax.experimental import pallas as pl
from jax.experimental.pallas import tpu as pltpu
from jax.sharding import Mesh
from jax.sharding import PartitionSpec as P


GRID_W = 64
EP = ("z", "core")
TP = ("y", "x")
EPS = 1e-06
BASE = 10000.0
LOG2E = 1.4426950408889634

bf16 = jnp.bfloat16
f32 = jnp.float32


def dot(a, b):
    return jnp.dot(a, b, preferred_element_type=f32)


def params(mib=16):
    return pltpu.CompilerParams(vmem_limit_bytes=mib << 20)


def start_copies(pairs, sems):
    copies = [pltpu.make_async_copy(a, b, sems.at[i]) for i, (a, b) in enumerate(pairs)]
    for copy in copies:
        copy.start()
    return copies


def norm_turn(x, gain, cos, sin):
    half = x.shape[0] // 2
    x = x * lax.rsqrt(jnp.mean(x * x, axis=0, keepdims=True) + EPS) * gain
    a, b = x[:half], x[half:]
    return jnp.concatenate([a * cos - b * sin, a * sin + b * cos], axis=0)


def column(row):
    n = row.shape[1]
    same = lax.broadcasted_iota(jnp.int32, (n, n), 0) == lax.broadcasted_iota(
        jnp.int32, (n, n), 1
    )
    return jnp.sum(jnp.where(same, row, 0.0), axis=1, keepdims=True)


def key_chunk(k_ref, v_ref, gain_ref, cos_ref, sin_ref, chunk_ref):
    hw, n = k_ref.shape
    k_t = norm_turn(k_ref[...].astype(f32), column(gain_ref[...]), cos_ref[...], sin_ref[...])
    k_t = k_t.astype(bf16).astype(f32)
    packed = jnp.concatenate([k_t[:, : n // 2], k_t[:, n // 2 :]], axis=0)
    chunk_ref[: n // 2, :] = packed.T.astype(bf16)
    for j in range(n // 128):
        chunk_ref[n // 2 + hw * j : n // 2 + hw * (j + 1), :] = v_ref[:, 128 * j : 128 * (j + 1)]


def query_body(q_ref, gain_ref, cos_ref, sin_ref, qt_ref):
    n = q_ref.shape[0]
    hw = gain_ref.shape[1]
    q_t = q_ref[...].astype(f32).T
    gain = column(gain_ref[...])
    for h in range(q_t.shape[0] // hw):
        turned = norm_turn(q_t[hw * h : hw * (h + 1)], gain, cos_ref[...], sin_ref[...])
        scaled = turned.astype(bf16).astype(f32) * (hw**-0.5)
        qt_ref[:, n * h : n * (h + 1)] = scaled.astype(bf16)


def attend_body(
    qt_ref, kv_ref, out_ref, qlo_ref, qhi_ref, m_ref, acc_ref, s_ref, p_ref, *, n, hw, tile
):
    step = pl.program_id(0)
    cols = qt_ref.shape[1]
    half = n // 2

    @pl.when(step == 0)
    def _():
        zero = jnp.zeros((hw, cols), bf16)
        scaled = qt_ref[...].astype(f32) * LOG2E
        big = scaled.astype(bf16)
        small = (scaled - big.astype(f32)).astype(bf16)
        for place, part in enumerate((big, zero, small, zero)):
            qlo_ref[hw * place : hw * (place + 1), :] = part
        for place, part in enumerate((zero, big, zero, small)):
            qhi_ref[hw * place : hw * (place + 1), :] = part
        m_ref[...] = jnp.full(m_ref.shape, -1e30, f32)
        acc_ref[...] = jnp.zeros(acc_ref.shape, f32)

    ones = jnp.ones((16, half), bf16)
    units = [(c, t) for c in range(kv_ref.shape[0] // n) for t in range(cols // tile)]
    shrink = {}

    def scores(u):
        c, t = units[u]
        at = pl.ds(tile * t, tile)
        k_pack = kv_ref[n * c : n * c + half, :]
        k_pack = jnp.concatenate([k_pack, k_pack], axis=1)
        s_ref[u % 2, :half, :] = dot(k_pack, qlo_ref[:, at])
        s_ref[u % 2, half:, :] = dot(k_pack, qhi_ref[:, at])

    def weights(u):
        at = pl.ds(tile * units[u][1], tile)
        s = s_ref[u % 2]
        old = m_ref[:, at]
        new = jnp.maximum(old, jnp.max(s, axis=0, keepdims=True))
        m_ref[:, at] = new
        shrink[u] = jnp.exp2(old - new)
        p_ref[u % 2] = jnp.exp2(s - new).astype(bf16)

    def values(u):
        c, t = units[u]
        at = pl.ds(tile * t, tile)
        base = n * c + half
        v = [kv_ref[base + hw * j : base + hw * (j + 1), :] for j in range(4)]
        v_a = jnp.concatenate([jnp.concatenate(v[:2], axis=1), ones], axis=0)
        v_b = jnp.concatenate([jnp.concatenate(v[2:], axis=1), ones], axis=0)
        term = dot(v_a, p_ref[u % 2, :half, :]) + dot(v_b, p_ref[u % 2, half:, :])
        acc_ref[:, at] = acc_ref[:, at] * shrink[u] + term

    for i in range(len(units) + 2):
        if i < len(units):
            scores(i)
        if i >= 2:
            values(i - 2)
        if 1 <= i <= len(units):
            weights(i - 1)

    @pl.when(step == pl.num_programs(0) - 1)
    def _():
        acc = acc_ref[...]
        out = acc[:hw] / acc[hw : hw + 1]
        heads = cols // n
        stacked = jnp.concatenate([out[:, n * h : n * (h + 1)] for h in range(heads)], axis=0)
        out_ref[...] = stacked.T.astype(bf16)


def weights_body(at_ref, w0, w1, w2, w3, after_ref, out_ref):
    del after_ref
    x = at_ref[1]
    count = out_ref.shape[0]
    width = out_ref.shape[1] // count
    base = w0.shape[0] - out_ref.shape[1]
    for j, w_ref in enumerate((w0, w1, w2, w3)):
        for d in range(count):
            row = pl.multiple_of(base + (x ^ d) * width, width)
            out_ref[j, width * d : width * (d + 1), :] = w_ref[pl.ds(row, width), :]


def mixer_body(a0, a1, a2, a3, w_ref, own_ref, p1_ref, p2_ref, p3_ref):
    near = jnp.concatenate([a0[...], a1[...]], axis=1)
    far = jnp.concatenate([a2[...], a3[...]], axis=1)
    half = near.shape[1]
    for j, out_ref in enumerate((own_ref, p1_ref, p2_ref, p3_ref)):
        acc = dot(near, w_ref[j, :half, :]) + dot(far, w_ref[j, half:, :])
        out_ref[...] = acc.astype(out_ref.dtype)


def mixed_body(own_ref, r1_ref, r2_ref, r3_ref, out_ref):
    total = own_ref[...]
    for ref in (r1_ref, r2_ref, r3_ref):
        total = total + ref[...].astype(f32)
    out_ref[...] = total.astype(bf16)


def front_body(at_ref, *refs, experts, cap):
    inputs, (chunk_ref, out_ref), held, sems = refs[:8], refs[8:10], refs[10:18], refs[18]
    copies = start_copies(tuple(zip(inputs, held)), sems)
    x_ref, gain_ref, routes_ref = held[5:]
    for copy in copies[:5]:
        copy.wait()
    key_chunk(*held[:5], chunk_ref)
    rows = x_ref.shape[0]
    copies[7].wait()
    ids = lax.broadcasted_iota(jnp.int32, (experts, rows), 0)
    hits = jnp.zeros((experts, rows), f32)
    for k in range(routes_ref.shape[0]):
        hits = hits + (ids == routes_ref[k : k + 1, :]).astype(f32)
    before = lax.broadcasted_iota(jnp.int32, (rows, rows), 0) < lax.broadcasted_iota(
        jnp.int32, (rows, rows), 1
    )
    rank = dot(hits.astype(bf16), before.astype(f32).astype(bf16))
    marks = (hits * (rank + 1.0)).astype(bf16)
    slots = experts * cap
    slot_row = lax.broadcasted_iota(jnp.int32, (slots, experts), 0)
    slot_exp = lax.broadcasted_iota(jnp.int32, (slots, experts), 1)
    spread = ((slot_row >= slot_exp * cap) & (slot_row < (slot_exp + 1) * cap)).astype(f32)
    wide = dot(spread.astype(bf16), marks)
    place = lax.broadcasted_iota(jnp.int32, (slots, rows), 0)
    want = (lax.rem(place, jnp.full_like(place, cap)) + 1).astype(f32)
    pick = (wide == want).astype(f32).astype(bf16)
    copies[5].wait()
    copies[6].wait()
    x = x_ref[...].astype(f32)
    width = out_ref.shape[1]
    own = pl.ds(pl.multiple_of(at_ref[0] * width, width), width)
    scale = lax.rsqrt(jnp.mean(x * x, axis=-1, keepdims=True) + EPS)
    normed = (x_ref[:, own].astype(f32) * scale * gain_ref[:, own]).astype(bf16)
    out_ref[...] = dot(pick, normed).astype(bf16)


def pack_body(at_ref, gate_ref, up_ref, mixer_ref, *out_refs):
    y = at_ref[0]
    count = len(out_refs)
    hid, width = gate_ref.shape[0], out_refs[0].shape[1]
    deep, rows = gate_ref.shape[1] // count, mixer_ref.shape[0] // count
    for d, out_ref in enumerate(out_refs):
        row = lax.rem(y + count - d, count)
        for b in range(deep // width):
            at = pl.ds(pl.multiple_of(row * deep + b * width, width), width)
            out_ref[2 * hid * b : 2 * hid * b + hid, :] = gate_ref[:, at]
            out_ref[2 * hid * b + hid : 2 * hid * (b + 1), :] = up_ref[:, at]
        out_ref[2 * hid * deep // width :, :] = mixer_ref[pl.ds(pl.multiple_of(row * rows, rows), rows), :]


def spread_body(x_ref, *refs):
    out_ref = refs[-1]
    cores, copies = 2, out_ref.shape[0] // 2
    count, rows, width = x_ref.shape
    cap = rows // cores
    x = x_ref[...].astype(f32)
    for c in range(cores):
        part = x[:, cap * c : cap * (c + 1), :].reshape(count * cap, width).astype(bf16)
        for i in range(copies):
            out_ref[copies * c + i] = part


def gate_up_body(at_ref, x_ref, w0_ref, w1_ref, w2_ref, w3_ref, out_ref):
    _, rows, _ = x_ref.shape
    y = at_ref[0]
    ws = (w0_ref, w1_ref, w2_ref, w3_ref)
    hid = out_ref.shape[2]
    blocks = x_ref.shape[0] // 2
    for j in range(0, len(ws), 2):
        for c in range(2):
            acc = None
            for b in range(blocks):
                at = slice(hid * b, hid * (b + 1))
                w = jnp.concatenate([ws[j][at, :], ws[j + 1][at, :]], axis=0)
                term = lax.dot_general(
                    x_ref[blocks * c + b], w, (((1,), (1,)), ((), ())), preferred_element_type=f32
                )
                acc = term if acc is None else acc + term
            at = slice(rows * c, rows * (c + 1))
            out_ref[lax.rem(y + j, len(ws)), at, :] = acc[:, :hid].astype(bf16)
            out_ref[lax.rem(y + j + 1, len(ws)), at, :] = acc[:, hid:].astype(bf16)


def hidden_body(parts_ref, out_ref):
    total = parts_ref[0].astype(f32)
    for j in range(1, parts_ref.shape[0]):
        total = total + parts_ref[j].astype(f32)
    hid = total.shape[1] // 2
    gate = total
    up = pltpu.roll(total, hid, 1)
    value = gate / (1.0 + jnp.exp(-gate)) * up
    rows = total.shape[0] // 2
    low = lax.broadcasted_iota(jnp.int32, (rows, 2 * hid), 1) < hid
    packed = jnp.where(low, value[:rows], pltpu.roll(value[rows:], hid, 1)).astype(bf16)
    for i in range(out_ref.shape[0]):
        out_ref[i] = packed


def down_body(h_ref, w_ref, after_ref, out_ref, wlo_ref, whi_ref):
    del after_ref
    count, _, width = h_ref.shape
    hid = width // 2
    zero = jnp.zeros((hid, w_ref.shape[1]), bf16)
    for j in range(count):
        part = w_ref[hid * j : hid * (j + 1), :]
        wlo_ref[width * j : width * j + hid, :] = part
        wlo_ref[width * j + hid : width * (j + 1), :] = zero
        whi_ref[width * j : width * j + hid, :] = zero
        whi_ref[width * j + hid : width * (j + 1), :] = part
    top = bottom = None
    for j in range(0, count, 2):
        pair = jnp.concatenate([h_ref[j], h_ref[j + 1]], axis=1)
        a = dot(pair, wlo_ref[width * j : width * (j + 2), :])
        b = dot(pair, whi_ref[width * j : width * (j + 2), :])
        top = a if top is None else top + a
        bottom = b if bottom is None else bottom + b
    groups, both, width = out_ref.shape
    cap = both // 2
    out_ref[:, :cap, :] = top.reshape(groups, cap, width).astype(bf16)
    out_ref[:, cap:, :] = bottom.reshape(groups, cap, width).astype(bf16)


def routing_body(routes_ref, weight_ref, pick_ref, share_ref, *, experts, cap):
    top_k, rows = routes_ref.shape
    both = jnp.concatenate(
        [routes_ref[...].astype(f32), weight_ref[...], jnp.zeros((128 - 2 * top_k, rows), f32)],
        axis=0,
    ).T
    named = [both[:, k : k + 1].astype(jnp.int32) for k in range(top_k)]
    ids = lax.broadcasted_iota(jnp.int32, (rows, experts), 1)
    each = [(ids == name).astype(f32) for name in named]
    hits = each[0]
    total = both[:, top_k : top_k + 1]
    for k in range(1, top_k):
        hits = hits + each[k]
        total = total + both[:, top_k + k : top_k + k + 1]
    before = lax.broadcasted_iota(jnp.int32, (rows, rows), 1) < lax.broadcasted_iota(
        jnp.int32, (rows, rows), 0
    )
    rank = dot(before.astype(f32).astype(bf16), hits.astype(bf16))
    lane = lax.broadcasted_iota(jnp.int32, (rows, experts * cap), 1)
    for k in range(top_k):
        own_rank = jnp.sum(rank * each[k], axis=-1, keepdims=True).astype(jnp.int32)
        place = named[k] * cap + own_rank
        pick_ref[k] = (lane == place).astype(f32).astype(bf16)
        share = both[:, top_k + k : top_k + k + 1] / total
        share_ref[k] = jnp.broadcast_to(share, share_ref.shape[1:])


def combine_body(back_ref, pick_ref, share_ref, out_ref):
    back = back_ref[...]
    out = None
    for k in range(pick_ref.shape[0]):
        share = share_ref[k]
        share = jnp.concatenate([share] * (back.shape[1] // share.shape[1]), axis=1)
        term = dot(pick_ref[k], back) * share
        out = term if out is None else out + term
    out_ref[...] = out.astype(bf16)


def on_device(
    query_input,
    key_input,
    value_input,
    query_gain,
    key_gain,
    mixer_out,
    moe_input,
    moe_gain,
    routes,
    route_weight,
    expert_gate,
    expert_up,
    expert_down,
):
    seq, q_cols = query_input.shape
    hw = query_gain.shape[0]
    tokens, model = moe_input.shape
    tp = lax.axis_size(TP)
    ep = lax.axis_size(EP)
    ny = lax.axis_size("y")
    nx = lax.axis_size("x")
    width = model // tp
    experts = ep
    cap = 3 * tokens * routes.shape[1] // (2 * experts)
    slots = experts * cap
    hid = expert_gate.shape[2]

    at_y, at_x = lax.axis_index("y"), lax.axis_index("x")
    at_yx = jnp.stack([at_y, at_x]).astype(jnp.int32)
    smem = pl.BlockSpec(memory_space=pltpu.SMEM)
    vmem = pl.BlockSpec(memory_space=pltpu.VMEM)
    hbm = pl.BlockSpec(memory_space=pltpu.HBM)
    anywhere = pl.BlockSpec(memory_space=pl.ANY)

    positions = lax.axis_index(EP) * seq + jnp.arange(seq, dtype=jnp.int32)
    quarter = hw // 4
    inverse = BASE ** (-jnp.arange(quarter, dtype=f32) / quarter)
    row = (positions // GRID_W).astype(f32)
    col = (positions % GRID_W).astype(f32)
    angles = jnp.concatenate(
        [inverse[:, None] * row[None, :], inverse[:, None] * col[None, :]], axis=0
    )
    cos, sin = jnp.cos(angles), jnp.sin(angles)
    held = (
        key_input.T,
        value_input.T,
        key_gain[None, :],
        cos,
        sin,
        moe_input,
        moe_gain[None, :],
        routes.T,
    )
    chunk, own = pl.pallas_call(
        lambda *refs: front_body(*refs, experts=experts, cap=cap),
        out_shape=(
            jax.ShapeDtypeStruct((seq, 2 * hw), bf16),
            jax.ShapeDtypeStruct((slots, width), bf16),
        ),
        in_specs=[smem] + [hbm] * len(held),
        scratch_shapes=[pltpu.VMEM(a.shape, a.dtype) for a in held]
        + [pltpu.SemaphoreType.DMA((len(held),))],
        compiler_params=params(60),
        name="front",
    )(lax.axis_index(TP)[None].astype(jnp.int32), *held)
    keys = lax.all_gather(chunk, EP, axis=0, tiled=True)

    nz = lax.axis_size("z")
    received = lax.all_to_all(
        own.reshape(nz, 2 * cap, width), "z", split_axis=0, concat_axis=0, tiled=True
    )

    q_t = pl.pallas_call(
        query_body,
        out_shape=jax.ShapeDtypeStruct((hw, seq * q_cols // hw), bf16),
        compiler_params=params(),
        name="queries",
    )(query_input, query_gain[None, :], cos, sin)
    rows_y = mixer_out.shape[0] // ny
    packs = pl.pallas_call(
        pack_body,
        out_shape=[jax.ShapeDtypeStruct((2 * hid * nx + rows_y, width), bf16)] * ny,
        in_specs=[smem] + [vmem] * 3,
        compiler_params=params(),
        name="pack",
    )(at_yx, expert_gate[0].T, expert_up[0].T, mixer_out)
    moved = [packs[0]]
    for d in range(1, ny):
        moved.append(lax.ppermute(packs[d], "y", [(i, (i - d) % ny) for i in range(ny)]))
    pick, share = pl.pallas_call(
        lambda *refs: routing_body(*refs, experts=experts, cap=cap),
        out_shape=(
            jax.ShapeDtypeStruct((routes.shape[1], tokens, slots), bf16),
            jax.ShapeDtypeStruct((routes.shape[1], tokens, 128), f32),
        ),
        compiler_params=params(),
        name="routing",
    )(routes.T, route_weight.T)

    block = pl.pallas_call(
        spread_body,
        out_shape=jax.ShapeDtypeStruct((2 * nx, slots // 2, width), bf16),
        in_specs=[vmem] + [anywhere] * 3,
        compiler_params=params(),
        name="spread",
    )(received, q_t, pick, packs[0][:8, :128])
    block = lax.all_to_all(block, ("core", "x"), split_axis=0, concat_axis=0, tiled=True)
    partial = pl.pallas_call(
        gate_up_body,
        out_shape=jax.ShapeDtypeStruct((ny, slots, 2 * hid), bf16),
        in_specs=[smem] + [vmem] * 5,
        compiler_params=params(),
        name="gate_up",
    )(at_yx, block, *moved)
    partial = lax.all_to_all(partial, "y", split_axis=0, concat_axis=0, tiled=True)
    hidden = pl.pallas_call(
        hidden_body,
        out_shape=jax.ShapeDtypeStruct((tp, slots // 2, 2 * hid), bf16),
        compiler_params=params(),
        name="hidden",
    )(partial)
    all_hidden = lax.all_to_all(hidden, TP, split_axis=0, concat_axis=0, tiled=True)

    step_rows = 16 * seq
    attended = pl.pallas_call(
        lambda *refs: attend_body(*refs, n=seq, hw=hw, tile=256),
        out_shape=jax.ShapeDtypeStruct((seq, q_cols), bf16),
        grid=(ep * seq // step_rows,),
        in_specs=[
            pl.BlockSpec(q_t.shape, lambda i: (0, 0)),
            pl.BlockSpec((step_rows, 2 * hw), lambda i: (i, 0)),
        ],
        out_specs=pl.BlockSpec((seq, q_cols), lambda i: (0, 0)),
        scratch_shapes=[
            pltpu.VMEM((4 * hw, q_t.shape[1]), bf16),
            pltpu.VMEM((4 * hw, q_t.shape[1]), bf16),
            pltpu.VMEM((1, q_t.shape[1]), f32),
            pltpu.VMEM((hw + 16, q_t.shape[1]), f32),
            pltpu.VMEM((2, seq, 256), f32),
            pltpu.VMEM((2, seq, 256), bf16),
        ],
        compiler_params=params(32),
        cost_estimate=pl.CostEstimate(
            flops=4 * seq * seq * ep * q_cols, bytes_accessed=4 << 20, transcendentals=0
        ),
        name="attend",
    )(q_t, keys)
    parts = [attended]
    for d in range(1, nx):
        parts.append(lax.ppermute(attended, "x", [(i, i ^ d) for i in range(nx)]))

    expert_out = pl.pallas_call(
        down_body,
        out_shape=jax.ShapeDtypeStruct((nz, 2 * cap, width), bf16),
        in_specs=[vmem, vmem, anywhere],
        scratch_shapes=[
            pltpu.VMEM((2 * hid * tp, width), bf16),
            pltpu.VMEM((2 * hid * tp, width), bf16),
        ],
        compiler_params=params(),
        name="down",
    )(all_hidden, expert_down[0], attended)
    returned = lax.all_to_all(
        expert_out.reshape(ep, cap, width), EP, split_axis=0, concat_axis=0, tiled=True
    ).reshape(slots, width)

    features = mixer_out.shape[1]
    turned = pl.pallas_call(
        weights_body,
        out_shape=jax.ShapeDtypeStruct((ny, rows_y, features), bf16),
        in_specs=[smem] + [vmem] * 4 + [anywhere],
        compiler_params=params(),
        name="weights",
    )(at_yx, *moved, attended[:8, :])
    mixed = pl.pallas_call(
        mixer_body,
        out_shape=[jax.ShapeDtypeStruct((seq, features), f32)]
        + [jax.ShapeDtypeStruct((seq, features), bf16)] * (ny - 1),
        compiler_params=params(),
        name="mixer",
    )(*parts, turned)
    sums = [mixed[0]]
    for d in range(1, ny):
        sums.append(lax.ppermute(mixed[d], "y", [(i, (i + d) % ny) for i in range(ny)]))
    attn_mixed = pl.pallas_call(
        mixed_body,
        out_shape=jax.ShapeDtypeStruct((seq, features), bf16),
        compiler_params=params(),
        name="mixed",
    )(*sums)

    moe_out = pl.pallas_call(
        combine_body,
        out_shape=jax.ShapeDtypeStruct((tokens, width), bf16),
        compiler_params=params(),
        name="combine",
    )(returned, pick, share)
    return (attn_mixed, moe_out)


def solution(mesh):
    torus = Mesh(mesh.devices.reshape(mesh.shape["ep"] // 2, 2, 4, 4), (*EP, *TP))
    placed = (
        P(EP, TP),
        P(EP, TP),
        P(EP, TP),
        P(),
        P(),
        P(None, TP),
        P(EP, None),
        P(),
        P(EP, None),
        P(EP, None),
        P(EP, None, TP),
        P(EP, None, TP),
        P(EP, None, TP),
    )

    return jax.shard_map(
        on_device,
        mesh=torus,
        in_specs=placed,
        out_specs=(P(EP, TP), P(EP, TP)),
        check_vma=False,
    )
```

```python
import jax
import jax.numpy as jnp
from jax import lax
from jax.experimental import pallas as pl
from jax.experimental.pallas import tpu as pltpu
from jax.sharding import Mesh
from jax.sharding import PartitionSpec as P


GRID_W = 64
EP = ("z", "core")
TP = ("y", "x")
EPS = 1e-06
BASE = 10000.0
LOG2E = 1.4426950408889634

bf16 = jnp.bfloat16
f32 = jnp.float32


def dot(a, b):
    return jnp.dot(a, b, preferred_element_type=f32)


def params(mib=16):
    return pltpu.CompilerParams(vmem_limit_bytes=mib << 20)


def start_copies(pairs, sems):
    copies = [pltpu.make_async_copy(a, b, sems.at[i]) for i, (a, b) in enumerate(pairs)]
    for copy in copies:
        copy.start()
    return copies


def norm_turn(x, gain, cos, sin):
    half = x.shape[0] // 2
    x = x * lax.rsqrt(jnp.mean(x * x, axis=0, keepdims=True) + EPS) * gain
    a, b = x[:half], x[half:]
    return jnp.concatenate([a * cos - b * sin, a * sin + b * cos], axis=0)


def column(row):
    n = row.shape[1]
    same = lax.broadcasted_iota(jnp.int32, (n, n), 0) == lax.broadcasted_iota(
        jnp.int32, (n, n), 1
    )
    return jnp.sum(jnp.where(same, row, 0.0), axis=1, keepdims=True)


def key_chunk(k_ref, v_ref, gain_ref, cos_ref, sin_ref, chunk_ref):
    hw, n = k_ref.shape
    k_t = norm_turn(k_ref[...].astype(f32), column(gain_ref[...]), cos_ref[...], sin_ref[...])
    k_t = k_t.astype(bf16).astype(f32)
    packed = jnp.concatenate([k_t[:, : n // 2], k_t[:, n // 2 :]], axis=0)
    chunk_ref[: n // 2, :] = packed.T.astype(bf16)
    for j in range(n // 128):
        chunk_ref[n // 2 + hw * j : n // 2 + hw * (j + 1), :] = v_ref[:, 128 * j : 128 * (j + 1)]


def query_body(q_ref, gain_ref, cos_ref, sin_ref, qt_ref):
    n = q_ref.shape[0]
    hw = gain_ref.shape[1]
    q_t = q_ref[...].astype(f32).T
    gain = column(gain_ref[...])
    for h in range(q_t.shape[0] // hw):
        turned = norm_turn(q_t[hw * h : hw * (h + 1)], gain, cos_ref[...], sin_ref[...])
        scaled = turned.astype(bf16).astype(f32) * (hw**-0.5)
        qt_ref[:, n * h : n * (h + 1)] = scaled.astype(bf16)


def attend_body(
    qt_ref, kv_ref, out_ref, qlo_ref, qhi_ref, m_ref, acc_ref, s_ref, p_ref, *, n, hw, tile
):
    step = pl.program_id(0)
    cols = qt_ref.shape[1]
    half = n // 2

    @pl.when(step == 0)
    def _():
        zero = jnp.zeros((hw, cols), bf16)
        scaled = qt_ref[...].astype(f32) * LOG2E
        big = scaled.astype(bf16)
        small = (scaled - big.astype(f32)).astype(bf16)
        for place, part in enumerate((big, zero, small, zero)):
            qlo_ref[hw * place : hw * (place + 1), :] = part
        for place, part in enumerate((zero, big, zero, small)):
            qhi_ref[hw * place : hw * (place + 1), :] = part
        m_ref[...] = jnp.full(m_ref.shape, -1e30, f32)
        acc_ref[...] = jnp.zeros(acc_ref.shape, f32)

    ones = jnp.ones((16, half), bf16)
    units = [(c, t) for c in range(kv_ref.shape[0] // n) for t in range(cols // tile)]
    shrink = {}

    def scores(u):
        c, t = units[u]
        at = pl.ds(tile * t, tile)
        k_pack = kv_ref[n * c : n * c + half, :]
        k_pack = jnp.concatenate([k_pack, k_pack], axis=1)
        s_ref[u % 2, :half, :] = dot(k_pack, qlo_ref[:, at])
        s_ref[u % 2, half:, :] = dot(k_pack, qhi_ref[:, at])

    def weights(u):
        at = pl.ds(tile * units[u][1], tile)
        s = s_ref[u % 2]
        old = m_ref[:, at]
        new = jnp.maximum(old, jnp.max(s, axis=0, keepdims=True))
        m_ref[:, at] = new
        shrink[u] = jnp.exp2(old - new)
        p_ref[u % 2] = jnp.exp2(s - new).astype(bf16)

    def values(u):
        c, t = units[u]
        at = pl.ds(tile * t, tile)
        base = n * c + half
        v = [kv_ref[base + hw * j : base + hw * (j + 1), :] for j in range(4)]
        v_a = jnp.concatenate([jnp.concatenate(v[:2], axis=1), ones], axis=0)
        v_b = jnp.concatenate([jnp.concatenate(v[2:], axis=1), ones], axis=0)
        term = dot(v_a, p_ref[u % 2, :half, :]) + dot(v_b, p_ref[u % 2, half:, :])
        acc_ref[:, at] = acc_ref[:, at] * shrink[u] + term

    for i in range(len(units) + 2):
        if i < len(units):
            scores(i)
        if i >= 2:
            values(i - 2)
        if 1 <= i <= len(units):
            weights(i - 1)

    @pl.when(step == pl.num_programs(0) - 1)
    def _():
        acc = acc_ref[...]
        out = acc[:hw] / acc[hw : hw + 1]
        heads = cols // n
        stacked = jnp.concatenate([out[:, n * h : n * (h + 1)] for h in range(heads)], axis=0)
        out_ref[...] = stacked.T.astype(bf16)


def weights_body(at_ref, w0, w1, w2, w3, after_ref, out_ref):
    del after_ref
    x = at_ref[1]
    count = out_ref.shape[0]
    width = out_ref.shape[1] // count
    base = w0.shape[0] - out_ref.shape[1]
    for j, w_ref in enumerate((w0, w1, w2, w3)):
        for d in range(count):
            row = pl.multiple_of(base + (x ^ d) * width, width)
            out_ref[j, width * d : width * (d + 1), :] = w_ref[pl.ds(row, width), :]


def mixer_body(a0, a1, a2, a3, w_ref, own_ref, p1_ref, p2_ref, p3_ref):
    near = jnp.concatenate([a0[...], a1[...]], axis=1)
    far = jnp.concatenate([a2[...], a3[...]], axis=1)
    half = near.shape[1]
    for j, out_ref in enumerate((own_ref, p1_ref, p2_ref, p3_ref)):
        acc = dot(near, w_ref[j, :half, :]) + dot(far, w_ref[j, half:, :])
        out_ref[...] = acc.astype(out_ref.dtype)


def mixed_body(own_ref, r1_ref, r2_ref, r3_ref, after_ref, out_ref):
    del after_ref
    total = own_ref[...]
    for ref in (r1_ref, r2_ref, r3_ref):
        total = total + ref[...].astype(f32)
    out_ref[...] = total.astype(bf16)


def front_body(at_ref, *refs, experts, cap):
    inputs, (chunk_ref, out_ref), held, sems = refs[:8], refs[8:10], refs[10:18], refs[18]
    copies = start_copies(tuple(zip(inputs, held)), sems)
    x_ref, gain_ref, routes_ref = held[5:]
    for copy in copies[:5]:
        copy.wait()
    key_chunk(*held[:5], chunk_ref)
    rows = x_ref.shape[0]
    copies[7].wait()
    ids = lax.broadcasted_iota(jnp.int32, (experts, rows), 0)
    hits = jnp.zeros((experts, rows), f32)
    for k in range(routes_ref.shape[0]):
        hits = hits + (ids == routes_ref[k : k + 1, :]).astype(f32)
    before = lax.broadcasted_iota(jnp.int32, (rows, rows), 0) < lax.broadcasted_iota(
        jnp.int32, (rows, rows), 1
    )
    rank = dot(hits.astype(bf16), before.astype(f32).astype(bf16))
    marks = (hits * (rank + 1.0)).astype(bf16)
    slots = experts * cap
    slot_row = lax.broadcasted_iota(jnp.int32, (slots, experts), 0)
    slot_exp = lax.broadcasted_iota(jnp.int32, (slots, experts), 1)
    spread = ((slot_row >= slot_exp * cap) & (slot_row < (slot_exp + 1) * cap)).astype(f32)
    wide = dot(spread.astype(bf16), marks)
    place = lax.broadcasted_iota(jnp.int32, (slots, rows), 0)
    want = (lax.rem(place, jnp.full_like(place, cap)) + 1).astype(f32)
    pick = (wide == want).astype(f32).astype(bf16)
    copies[5].wait()
    copies[6].wait()
    x = x_ref[...].astype(f32)
    width = out_ref.shape[1]
    own = pl.ds(pl.multiple_of(at_ref[0] * width, width), width)
    scale = lax.rsqrt(jnp.mean(x * x, axis=-1, keepdims=True) + EPS)
    normed = (x_ref[:, own].astype(f32) * scale * gain_ref[:, own]).astype(bf16)
    out_ref[...] = dot(pick, normed).astype(bf16)


def pack_body(at_ref, gate_ref, up_ref, mixer_ref, *out_refs):
    y = at_ref[0]
    count = len(out_refs)
    hid, width = gate_ref.shape[0], out_refs[0].shape[1]
    deep, rows = gate_ref.shape[1] // count, mixer_ref.shape[0] // count
    for d, out_ref in enumerate(out_refs):
        row = lax.rem(y + count - d, count)
        for b in range(deep // width):
            at = pl.ds(pl.multiple_of(row * deep + b * width, width), width)
            out_ref[2 * hid * b : 2 * hid * b + hid, :] = gate_ref[:, at]
            out_ref[2 * hid * b + hid : 2 * hid * (b + 1), :] = up_ref[:, at]
        out_ref[2 * hid * deep // width :, :] = mixer_ref[pl.ds(pl.multiple_of(row * rows, rows), rows), :]


def spread_body(x_ref, *refs):
    out_ref = refs[-1]
    cores, copies = 2, out_ref.shape[0] // 2
    count, rows, width = x_ref.shape
    cap = rows // cores
    x = x_ref[...].astype(f32)
    for c in range(cores):
        part = x[:, cap * c : cap * (c + 1), :].reshape(count * cap, width).astype(bf16)
        for i in range(copies):
            out_ref[copies * c + i] = part


def gate_up_body(at_ref, x_ref, w0_ref, w1_ref, w2_ref, w3_ref, out_ref):
    _, rows, _ = x_ref.shape
    y = at_ref[0]
    ws = (w0_ref, w1_ref, w2_ref, w3_ref)
    hid = out_ref.shape[2]
    blocks = x_ref.shape[0] // 2
    for j in range(0, len(ws), 2):
        for c in range(2):
            acc = None
            for b in range(blocks):
                at = slice(hid * b, hid * (b + 1))
                w = jnp.concatenate([ws[j][at, :], ws[j + 1][at, :]], axis=0)
                term = lax.dot_general(
                    x_ref[blocks * c + b], w, (((1,), (1,)), ((), ())), preferred_element_type=f32
                )
                acc = term if acc is None else acc + term
            at = slice(rows * c, rows * (c + 1))
            out_ref[lax.rem(y + j, len(ws)), at, :] = acc[:, :hid].astype(bf16)
            out_ref[lax.rem(y + j + 1, len(ws)), at, :] = acc[:, hid:].astype(bf16)


def hidden_body(parts_ref, out_ref):
    total = parts_ref[0].astype(f32)
    for j in range(1, parts_ref.shape[0]):
        total = total + parts_ref[j].astype(f32)
    hid = total.shape[1] // 2
    gate = total
    up = pltpu.roll(total, hid, 1)
    value = gate / (1.0 + jnp.exp(-gate)) * up
    rows = total.shape[0] // 2
    low = lax.broadcasted_iota(jnp.int32, (rows, 2 * hid), 1) < hid
    packed = jnp.where(low, value[:rows], pltpu.roll(value[rows:], hid, 1)).astype(bf16)
    for i in range(out_ref.shape[0]):
        out_ref[i] = packed


def down_body(h_ref, w_ref, after_ref, out_ref, wlo_ref, whi_ref):
    del after_ref
    count, _, width = h_ref.shape
    hid = width // 2
    zero = jnp.zeros((hid, w_ref.shape[1]), bf16)
    for j in range(count):
        part = w_ref[hid * j : hid * (j + 1), :]
        wlo_ref[width * j : width * j + hid, :] = part
        wlo_ref[width * j + hid : width * (j + 1), :] = zero
        whi_ref[width * j : width * j + hid, :] = zero
        whi_ref[width * j + hid : width * (j + 1), :] = part
    top = bottom = None
    for j in range(0, count, 2):
        pair = jnp.concatenate([h_ref[j], h_ref[j + 1]], axis=1)
        a = dot(pair, wlo_ref[width * j : width * (j + 2), :])
        b = dot(pair, whi_ref[width * j : width * (j + 2), :])
        top = a if top is None else top + a
        bottom = b if bottom is None else bottom + b
    groups, both, width = out_ref.shape
    cap = both // 2
    out_ref[:, :cap, :] = top.reshape(groups, cap, width).astype(bf16)
    out_ref[:, cap:, :] = bottom.reshape(groups, cap, width).astype(bf16)


def routing_body(routes_ref, weight_ref, pick_ref, share_ref, *, experts, cap):
    top_k, rows = routes_ref.shape
    both = jnp.concatenate(
        [routes_ref[...].astype(f32), weight_ref[...], jnp.zeros((128 - 2 * top_k, rows), f32)],
        axis=0,
    ).T
    named = [both[:, k : k + 1].astype(jnp.int32) for k in range(top_k)]
    ids = lax.broadcasted_iota(jnp.int32, (rows, experts), 1)
    each = [(ids == name).astype(f32) for name in named]
    hits = each[0]
    total = both[:, top_k : top_k + 1]
    for k in range(1, top_k):
        hits = hits + each[k]
        total = total + both[:, top_k + k : top_k + k + 1]
    before = lax.broadcasted_iota(jnp.int32, (rows, rows), 1) < lax.broadcasted_iota(
        jnp.int32, (rows, rows), 0
    )
    rank = dot(before.astype(f32).astype(bf16), hits.astype(bf16))
    lane = lax.broadcasted_iota(jnp.int32, (rows, experts * cap), 1)
    for k in range(top_k):
        own_rank = jnp.sum(rank * each[k], axis=-1, keepdims=True).astype(jnp.int32)
        place = named[k] * cap + own_rank
        pick_ref[k] = (lane == place).astype(f32).astype(bf16)
        share = both[:, top_k + k : top_k + k + 1] / total
        share_ref[k] = jnp.broadcast_to(share, share_ref.shape[1:])


def combine_body(back_ref, pick_ref, share_ref, out_ref):
    back = back_ref[...]
    out = None
    for k in range(pick_ref.shape[0]):
        share = share_ref[k]
        share = jnp.concatenate([share] * (back.shape[1] // share.shape[1]), axis=1)
        term = dot(pick_ref[k], back) * share
        out = term if out is None else out + term
    out_ref[...] = out.astype(bf16)


def on_device(
    query_input,
    key_input,
    value_input,
    query_gain,
    key_gain,
    mixer_out,
    moe_input,
    moe_gain,
    routes,
    route_weight,
    expert_gate,
    expert_up,
    expert_down,
):
    seq, q_cols = query_input.shape
    hw = query_gain.shape[0]
    tokens, model = moe_input.shape
    tp = lax.axis_size(TP)
    ep = lax.axis_size(EP)
    ny = lax.axis_size("y")
    nx = lax.axis_size("x")
    width = model // tp
    experts = ep
    cap = 3 * tokens * routes.shape[1] // (2 * experts)
    slots = experts * cap
    hid = expert_gate.shape[2]

    at_y, at_x = lax.axis_index("y"), lax.axis_index("x")
    at_yx = jnp.stack([at_y, at_x]).astype(jnp.int32)
    smem = pl.BlockSpec(memory_space=pltpu.SMEM)
    vmem = pl.BlockSpec(memory_space=pltpu.VMEM)
    hbm = pl.BlockSpec(memory_space=pltpu.HBM)
    anywhere = pl.BlockSpec(memory_space=pl.ANY)

    positions = lax.axis_index(EP) * seq + jnp.arange(seq, dtype=jnp.int32)
    quarter = hw // 4
    inverse = BASE ** (-jnp.arange(quarter, dtype=f32) / quarter)
    row = (positions // GRID_W).astype(f32)
    col = (positions % GRID_W).astype(f32)
    angles = jnp.concatenate(
        [inverse[:, None] * row[None, :], inverse[:, None] * col[None, :]], axis=0
    )
    cos, sin = jnp.cos(angles), jnp.sin(angles)
    held = (
        key_input.T,
        value_input.T,
        key_gain[None, :],
        cos,
        sin,
        moe_input,
        moe_gain[None, :],
        routes.T,
    )
    chunk, own = pl.pallas_call(
        lambda *refs: front_body(*refs, experts=experts, cap=cap),
        out_shape=(
            jax.ShapeDtypeStruct((seq, 2 * hw), bf16),
            jax.ShapeDtypeStruct((slots, width), bf16),
        ),
        in_specs=[smem] + [hbm] * len(held),
        scratch_shapes=[pltpu.VMEM(a.shape, a.dtype) for a in held]
        + [pltpu.SemaphoreType.DMA((len(held),))],
        compiler_params=params(60),
        name="front",
    )(lax.axis_index(TP)[None].astype(jnp.int32), *held)
    keys = lax.all_gather(chunk, EP, axis=0, tiled=True)

    nz = lax.axis_size("z")
    received = lax.all_to_all(
        own.reshape(nz, 2 * cap, width), "z", split_axis=0, concat_axis=0, tiled=True
    )

    q_t = pl.pallas_call(
        query_body,
        out_shape=jax.ShapeDtypeStruct((hw, seq * q_cols // hw), bf16),
        compiler_params=params(),
        name="queries",
    )(query_input, query_gain[None, :], cos, sin)
    rows_y = mixer_out.shape[0] // ny
    packs = pl.pallas_call(
        pack_body,
        out_shape=[jax.ShapeDtypeStruct((2 * hid * nx + rows_y, width), bf16)] * ny,
        in_specs=[smem] + [vmem] * 3,
        compiler_params=params(),
        name="pack",
    )(at_yx, expert_gate[0].T, expert_up[0].T, mixer_out)
    moved = [packs[0]]
    for d in range(1, ny):
        moved.append(lax.ppermute(packs[d], "y", [(i, (i - d) % ny) for i in range(ny)]))
    pick, share = pl.pallas_call(
        lambda *refs: routing_body(*refs, experts=experts, cap=cap),
        out_shape=(
            jax.ShapeDtypeStruct((routes.shape[1], tokens, slots), bf16),
            jax.ShapeDtypeStruct((routes.shape[1], tokens, 128), f32),
        ),
        compiler_params=params(),
        name="routing",
    )(routes.T, route_weight.T)

    block = pl.pallas_call(
        spread_body,
        out_shape=jax.ShapeDtypeStruct((2 * nx, slots // 2, width), bf16),
        in_specs=[vmem] + [anywhere] * 3,
        compiler_params=params(),
        name="spread",
    )(received, q_t, pick, packs[0][:8, :128])
    block = lax.all_to_all(block, ("core", "x"), split_axis=0, concat_axis=0, tiled=True)
    partial = pl.pallas_call(
        gate_up_body,
        out_shape=jax.ShapeDtypeStruct((ny, slots, 2 * hid), bf16),
        in_specs=[smem] + [vmem] * 5,
        compiler_params=params(),
        name="gate_up",
    )(at_yx, block, *moved)
    partial = lax.all_to_all(partial, "y", split_axis=0, concat_axis=0, tiled=True)
    hidden = pl.pallas_call(
        hidden_body,
        out_shape=jax.ShapeDtypeStruct((tp, slots // 2, 2 * hid), bf16),
        compiler_params=params(),
        name="hidden",
    )(partial)
    all_hidden = lax.all_to_all(hidden, TP, split_axis=0, concat_axis=0, tiled=True)

    step_rows = 16 * seq
    attended = pl.pallas_call(
        lambda *refs: attend_body(*refs, n=seq, hw=hw, tile=256),
        out_shape=jax.ShapeDtypeStruct((seq, q_cols), bf16),
        grid=(ep * seq // step_rows,),
        in_specs=[
            pl.BlockSpec(q_t.shape, lambda i: (0, 0)),
            pl.BlockSpec((step_rows, 2 * hw), lambda i: (i, 0)),
        ],
        out_specs=pl.BlockSpec((seq, q_cols), lambda i: (0, 0)),
        scratch_shapes=[
            pltpu.VMEM((4 * hw, q_t.shape[1]), bf16),
            pltpu.VMEM((4 * hw, q_t.shape[1]), bf16),
            pltpu.VMEM((1, q_t.shape[1]), f32),
            pltpu.VMEM((hw + 16, q_t.shape[1]), f32),
            pltpu.VMEM((2, seq, 256), f32),
            pltpu.VMEM((2, seq, 256), bf16),
        ],
        compiler_params=params(32),
        cost_estimate=pl.CostEstimate(
            flops=4 * seq * seq * ep * q_cols, bytes_accessed=4 << 20, transcendentals=0
        ),
        name="attend",
    )(q_t, keys)
    parts = [attended]
    for d in range(1, nx):
        parts.append(lax.ppermute(attended, "x", [(i, i ^ d) for i in range(nx)]))

    expert_out = pl.pallas_call(
        down_body,
        out_shape=jax.ShapeDtypeStruct((nz, 2 * cap, width), bf16),
        in_specs=[vmem, vmem, anywhere],
        scratch_shapes=[
            pltpu.VMEM((2 * hid * tp, width), bf16),
            pltpu.VMEM((2 * hid * tp, width), bf16),
        ],
        compiler_params=params(),
        name="down",
    )(all_hidden, expert_down[0], attended)
    returned = lax.all_to_all(
        expert_out.reshape(ep, cap, width), EP, split_axis=0, concat_axis=0, tiled=True
    ).reshape(slots, width)

    features = mixer_out.shape[1]
    turned = pl.pallas_call(
        weights_body,
        out_shape=jax.ShapeDtypeStruct((ny, rows_y, features), bf16),
        in_specs=[smem] + [vmem] * 4 + [anywhere],
        compiler_params=params(),
        name="weights",
    )(at_yx, *moved, attended[:8, :])
    mixed = pl.pallas_call(
        mixer_body,
        out_shape=[jax.ShapeDtypeStruct((seq, features), f32)]
        + [jax.ShapeDtypeStruct((seq, features), bf16)] * (ny - 1),
        compiler_params=params(),
        name="mixer",
    )(*parts, turned)
    sums = [mixed[0]]
    for d in range(1, ny):
        sums.append(lax.ppermute(mixed[d], "y", [(i, (i + d) % ny) for i in range(ny)]))
    moe_out = pl.pallas_call(
        combine_body,
        out_shape=jax.ShapeDtypeStruct((tokens, width), bf16),
        compiler_params=params(),
        name="combine",
    )(returned, pick, share)
    attn_mixed = pl.pallas_call(
        mixed_body,
        out_shape=jax.ShapeDtypeStruct((seq, features), bf16),
        in_specs=[vmem] * 4 + [anywhere],
        compiler_params=params(),
        name="mixed",
    )(*sums, moe_out[:8, :128])

    return (attn_mixed, moe_out)


def solution(mesh):
    torus = Mesh(mesh.devices.reshape(mesh.shape["ep"] // 2, 2, 4, 4), (*EP, *TP))
    placed = (
        P(EP, TP),
        P(EP, TP),
        P(EP, TP),
        P(),
        P(),
        P(None, TP),
        P(EP, None),
        P(),
        P(EP, None),
        P(EP, None),
        P(EP, None, TP),
        P(EP, None, TP),
        P(EP, None, TP),
    )

    return jax.shard_map(
        on_device,
        mesh=torus,
        in_specs=placed,
        out_specs=(P(EP, TP), P(EP, TP)),
        check_vma=False,
    )
```
